256 devices in a mesh: grp: 2 (over y), sp: 32 (over z, core), tp: 4 (over x).
Axes of the slice: x: 4, y: 2, z: 16, core: 2. Of those that a mesh axis runs over, the one named last changes fastest.
The devices are a block of a 4x16x16 slice.
Arguments:
- residual_in: bfloat16 [16384, 2048], P(('grp', 'sp', 'tp')), parts along dimension 0, may hold values from -1.1953125 to 1.1953125
- query_small: bfloat16 [16384, 1024], P(('grp', 'sp'), 'tp'), parts along dimension 0, may hold values from -6 to 6
- query_large: bfloat16 [16384, 1024], P(('grp', 'sp'), 'tp'), parts along dimension 0, may hold values from -6 to 6
- key_small: bfloat16 [64, 16384], P(None, ('grp', 'sp')), parts along dimension 1, may hold values from -6 to 6
- key_large: bfloat16 [128, 16384], P(None, ('grp', 'sp')), parts along dimension 1, may hold values from -6 to 6
- value_small: bfloat16 [64, 16384], P(None, ('grp', 'sp')), parts along dimension 1, may hold values from -6 to 6
- value_large: bfloat16 [128, 16384], P(None, ('grp', 'sp')), parts along dimension 1, may hold values from -6 to 6
- forget_small: float32 [16, 16384], P('tp', ('grp', 'sp')), parts along dimension 1, may hold values from -1172 to 0, as said below
- forget_large: float32 [8, 16384], P('tp', ('grp', 'sp')), parts along dimension 1, may hold values from -1172 to 0, as said below
- project_small: bfloat16 [1024, 2048], P('tp'), may hold values from -0.125 to 0.125
- project_large: bfloat16 [1024, 2048], P('tp'), may hold values from -0.125 to 0.125
- norm_gain: bfloat16 [2048], replicated, may hold values from 0.099609375 to 1.8984375
- expert_gate: bfloat16 [128, 2048, 512], P(('sp', 'tp')), may hold values from -0.125 to 0.125
- expert_up: bfloat16 [128, 2048, 512], P(('sp', 'tp')), may hold values from -0.125 to 0.125
- expert_down: bfloat16 [128, 512, 2048], P(('sp', 'tp')), may hold values from -0.25 to 0.25
- routing: int32 [16384, 2], P(('grp', 'sp', 'tp')), parts along dimension 0, may hold values from 0 to 127, all different within a row; in each aligned block of 64 rows (0 to 63, 64 to 127, ...) at most 2 rows name the same one
- route_weight: float32 [16384, 2], P(('grp', 'sp', 'tp')), parts along dimension 0, may hold values from 0.2 to 1
Outputs:
- layer_out: bfloat16 [16384, 2048], P(('grp', 'sp', 'tp')), parts along dimension 0
The draws below stay inside these ranges and needn't reach their ends.
There are 2 independent parts, one for each index of `grp`. The reference program is written for one: setup_inputs(seed, part) draws one part's arguments, and reference() takes and returns one part's arrays. A program takes and returns all parts, laid end to end along the dimension named above; an argument that names none is the same for every part. Nothing has to cross between parts.
Inputs may be any that keep to these rules, and one draw needn't show every extreme that they name: `forget_small`: each row never rises from one position to the next. `forget_large`: each row never rises from one position to the next. `routing`: each row names 2 different experts; in the rows of one device no expert is named by more than 2 rows, and in some devices' rows some expert is named by exactly 2.
All inputs are finite; a program needn't handle non-finite values.
Results may differ from the reference program's by a relative error of at most 0.018.
Values may be sent and summed in bfloat16 or wider, within the bound.
No kernel may reach another device: no remote copies, remote signals or barrier semaphores. Data moves between devices by JAX's collectives and lax.ppermute only.
A program may use at most 64 MiB of HBM per device.

```python
import math
import jax
import jax.numpy as jnp
import numpy as np
from jax import lax

D = 2048
HS_N = 16
DHS = 64
HL_N = 8
DHL = 128
FF = 512
TOP = 2
TOK_DEV = 256
SEQUENCE_TOKENS = 8192
ROWS = 64
EXPERTS = 128
CAP = 2
N_TP = 4


def query_draw(key, salt, number_heads, head_size):
    drawn = 1.5 * jax.random.truncated_normal(jax.random.fold_in(key, salt), -4.0, 4.0, (SEQUENCE_TOKENS, number_heads * head_size), jnp.float32)
    return drawn


def key_draw(key, salt, head_size):
    drawn = 1.5 * jax.random.truncated_normal(jax.random.fold_in(key, salt), -4.0, 4.0, (head_size, SEQUENCE_TOKENS), jnp.float32)
    return drawn


def gate_draw(key, salt, number_heads):
    root_random_key = jax.random.fold_in(key, salt)
    fast_share = 0.5
    is_fast = jax.random.uniform(jax.random.fold_in(root_random_key, 1), (number_heads,)) < fast_share
    slow_total = jnp.exp(jax.random.uniform(jax.random.fold_in(root_random_key, 2), (number_heads,), jnp.float32, math.log(0.3), math.log(0.8)))
    fast_rate = jnp.exp(-jax.random.uniform(jax.random.fold_in(root_random_key, 3), (number_heads,), jnp.float32, math.log(30.0), math.log(100.0)))
    rate = jnp.where(is_fast, fast_rate, slow_total / SEQUENCE_TOKENS)
    block_count = SEQUENCE_TOKENS // TOK_DEV
    block_factor = jnp.exp(jax.random.uniform(jax.random.fold_in(root_random_key, 4), (number_heads, block_count), jnp.float32, math.log(0.35), math.log(2.8)))
    block_factor = jnp.repeat(block_factor, TOK_DEV, axis=1)
    rough = jax.random.uniform(jax.random.fold_in(root_random_key, 5), (number_heads, SEQUENCE_TOKENS), jnp.float32, 0.5, 1.5)
    logarithm_gate = -rate[:, None] * block_factor * rough
    spike_position = jax.random.randint(jax.random.fold_in(root_random_key, 6), (number_heads, 2), 0, SEQUENCE_TOKENS)
    spike_penalty = -jnp.log(1.0 - jax.random.uniform(jax.random.fold_in(root_random_key, 7), (number_heads, 2), jnp.float32, 0.2, 0.4))
    per_head_rows = jnp.broadcast_to(jnp.arange(number_heads)[:, None], (number_heads, 2))
    logarithm_gate = logarithm_gate.at[per_head_rows, spike_position].add(-spike_penalty)
    return jnp.cumsum(logarithm_gate, axis=1)


def draw_query_small(key, part):
    return query_draw(key, 11, HS_N, DHS).astype(jnp.bfloat16)


def draw_query_large(key, part):
    return query_draw(key, 12, HL_N, DHL).astype(jnp.bfloat16)


def draw_key_small(key, part):
    return key_draw(key, 13, DHS).astype(jnp.bfloat16)


def draw_key_large(key, part):
    return key_draw(key, 14, DHL).astype(jnp.bfloat16)


def draw_forget_small(key, part):
    return gate_draw(key, 15, HS_N)


def draw_forget_large(key, part):
    return gate_draw(key, 16, HL_N)


def block_levels(rng, shape, pieces, low, largest):
    def one(dim, parts):
        heights = jax.random.uniform(jax.random.fold_in(jax.random.fold_in(rng, 6), dim), (parts,), jnp.float32, low / len(pieces), largest / len(pieces))
        return jnp.repeat(jnp.exp(heights), shape[dim] // parts).reshape((-1,) + (1,) * (len(shape) - dim - 1))

    factor_of = one(*pieces[0])
    for cut in pieces[1:]:
        factor_of = factor_of * one(*cut)
    return factor_of


def assign_block(rng, own, number, rows, number_of, top, bound, skew):
    order = jax.random.permutation(rng, number_of)
    packed, ordinary = shares(number_of, rows * top, bound, skew, True), shares(number_of, rows * top, bound, skew, False)
    places = jnp.arange(number_of)

    def named(sizes, rotation):
        used = int((sizes > 0).sum())
        fixed = max(1, used // 4)
        shifted = fixed + (places - fixed + rotation * (used - fixed)) % max(1, number_of - fixed)
        return jnp.zeros((number_of,), jnp.int32).at[order[jnp.where(places < fixed, places, shifted)]].set(jnp.asarray(sizes, jnp.int32))

    sizes = jnp.where(number % 4 == 0, named(packed, number // 4), named(ordinary, number - number // 4 - 1))
    mixed = jax.random.permutation(jax.random.fold_in(own, 3), number_of)
    giver, taker = mixed[0:number_of // 2 * 2:2], mixed[1:number_of // 2 * 2:2]
    room = jnp.minimum(sizes[giver] - 1, bound - sizes[taker]) // 2
    room = jnp.where((giver == order[0]) | (taker == order[0]) | (sizes[taker] == 0), 0, jnp.maximum(room, 0))
    shifted = jax.random.randint(jax.random.fold_in(own, 4), (number_of // 2,), 0, 1 << 20) % (room + 1)
    sizes = sizes.at[giver].add(-shifted).at[taker].add(shifted)
    labels = jnp.searchsorted(jnp.cumsum(sizes), jnp.arange(rows * top), side="right").astype(jnp.int32)
    grid = labels.reshape(top, rows).T
    grid = grid[jax.random.permutation(jax.random.fold_in(own, 1), rows)]
    rotation = jax.random.randint(jax.random.fold_in(own, 2), (rows, 1), 0, top)
    return jnp.take_along_axis(grid, (jnp.arange(top)[None, :] + rotation) % top, axis=1)


def shares(amount, total, bound, slope, full):
    portions = [(1 << 20) // math.isqrt(rank ** slope) + 1 for rank in range(1, amount + 1)]
    largest = bound if full else min(bound, max(-(-total // amount), total * portions[0] // sum(portions)))
    least = 1 if total - largest >= amount - 1 else 0
    holding, surplus = [largest] + [least] * (amount - 1), total - largest - least * (amount - 1)
    while surplus > 0:
        candidates = [i for i in range(1, amount) if holding[i] < largest] or [i for i in range(1, amount) if holding[i] < bound]
        mass, budget = sum([portions[i] for i in candidates]), surplus
        for i in candidates:
            extra = min(bound - holding[i], max(1, budget * portions[i] // mass), surplus)
            holding[i] = holding[i] + extra
            surplus = surplus - extra
    return np.array(holding)


def gaussian(key, extent, spread, limit, pieces=(), kind=jnp.bfloat16):
    level = block_levels(key, extent, pieces, -0.22, 0.18) if pieces else 1.0
    values = jax.random.normal(key, extent, jnp.float32) * spread * level
    return jnp.minimum(jnp.maximum(values, -limit), limit).astype(kind)


def setup_inputs(seed: int = 0, part: int = 0) -> dict:
    seeds = jax.random.split(jax.random.key(seed), 18)
    own_keys = jax.random.split(jax.random.fold_in(seeds[17], part), 18)
    residual_in = gaussian(own_keys[0], (SEQUENCE_TOKENS, D), 0.2, 1.1953125, ((0, 128),))
    query_small = draw_query_small(jax.random.fold_in(jax.random.fold_in(seeds[17], part), 71), part)
    query_large = draw_query_large(jax.random.fold_in(jax.random.fold_in(seeds[17], part), 71), part)
    key_small = draw_key_small(jax.random.fold_in(jax.random.fold_in(seeds[17], part), 71), part)
    key_large = draw_key_large(jax.random.fold_in(jax.random.fold_in(seeds[17], part), 71), part)
    value_small = gaussian(own_keys[5], (DHS, SEQUENCE_TOKENS), 1.0, 6.0, ((1, 32),))
    value_large = gaussian(own_keys[6], (DHL, SEQUENCE_TOKENS), 1.0, 6.0, ((1, 32),))
    forget_small = draw_forget_small(jax.random.fold_in(jax.random.fold_in(seeds[17], part), 71), part)
    forget_large = draw_forget_large(jax.random.fold_in(jax.random.fold_in(seeds[17], part), 71), part)
    project_small = gaussian(seeds[9], (HS_N * DHS, D), (HS_N * DHS + HL_N * DHL) ** -0.5, 0.125, ((0, 4),))
    project_large = gaussian(seeds[10], (HL_N * DHL, D), (HS_N * DHS + HL_N * DHL) ** -0.5, 0.125, ((0, 4),))
    norm_gain = jnp.clip(1.0 + 0.18 * jax.random.normal(seeds[11], (D,), jnp.float32), 0.099609375, 1.8984375).astype(jnp.bfloat16)
    expert_gate = gaussian(seeds[12], (EXPERTS, D, FF), D ** -0.5, 0.125, ((0, 128),))
    expert_up = gaussian(seeds[13], (EXPERTS, D, FF), D ** -0.5, 0.125, ((0, 128),))
    expert_down = gaussian(seeds[14], (EXPERTS, FF, D), FF ** -0.5, 0.25, ((0, 128),))
    routing_keys = jax.random.split(jax.random.fold_in(own_keys[15], 1), SEQUENCE_TOKENS // ROWS)
    routing_turns = jax.random.permutation(jax.random.fold_in(own_keys[15], 3), SEQUENCE_TOKENS // ROWS)
    routing = jax.vmap(lambda own, number: assign_block(jax.random.fold_in(own_keys[15], 2), own, number, ROWS, EXPERTS, TOP, CAP, 2))(routing_keys, routing_turns).reshape((SEQUENCE_TOKENS, TOP))
    route_weight = jnp.clip(0.2 + 0.8 * jax.random.uniform(own_keys[16], (SEQUENCE_TOKENS, TOP), jnp.float32) ** block_levels(own_keys[16], (SEQUENCE_TOKENS, TOP), ((0, 128),), -0.2, 0.2), 0.2, 1.0)
    return dict(residual_in=residual_in, query_small=query_small, query_large=query_large, key_small=key_small, key_large=key_large, value_small=value_small, value_large=value_large, forget_small=forget_small, forget_large=forget_large, project_small=project_small, project_large=project_large, norm_gain=norm_gain, expert_gate=expert_gate, expert_up=expert_up, expert_down=expert_down, routing=routing, route_weight=route_weight)


def attend(queries, keys_in, values_in, gates_in):
    number_heads = gates_in.shape[0]
    head_size = keys_in.shape[0]
    length = keys_in.shape[1]
    block_len = 512 if length % 512 == 0 else length
    results = []
    for block_index in range(length // block_len):
        first_row = block_index * block_len
        last_row = first_row + block_len
        query_rows = queries[first_row:last_row].reshape(block_len, number_heads, head_size).astype(jnp.float32)
        key_rows = keys_in[:, :last_row].astype(jnp.float32)
        value_rows = values_in[:, :last_row].astype(jnp.float32)
        scores = jnp.einsum('qhd,dk->hqk', query_rows, key_rows) * head_size ** (-0.5)
        scores = scores + gates_in[:, first_row:last_row, None] - gates_in[:, None, :last_row]
        causal = (jnp.arange(first_row, last_row)[:, None] >= jnp.arange(last_row)[None, :])[None]
        scores = jnp.where(causal, scores, -jnp.inf)
        row_top = lax.optimization_barrier(jnp.max(scores, axis=2, keepdims=True))
        weights = jnp.exp(scores - row_top)
        row_total = lax.optimization_barrier(jnp.sum(weights, axis=2))
        rounded = lax.optimization_barrier(weights.astype(jnp.bfloat16)).astype(jnp.float32)
        mixed = jnp.einsum('hqk,dk->qhd', rounded, value_rows) / row_total.T[:, :, None]
        results.append(mixed.reshape(block_len, number_heads * head_size).astype(jnp.bfloat16))
    return jnp.concatenate(results, axis=0)

def reference(residual_in, query_small, query_large, key_small, key_large, value_small, value_large, forget_small, forget_large, project_small, project_large, norm_gain, expert_gate, expert_up, expert_down, routing, route_weight):
    attn_small = attend(query_small, key_small, value_small, forget_small)
    attn_large = attend(query_large, key_large, value_large, forget_large)
    width_small = attn_small.shape[1] // N_TP
    width_large = attn_large.shape[1] // N_TP
    projected = jnp.zeros((SEQUENCE_TOKENS, D), jnp.float32)
    for member in range(N_TP):
        part_small = attn_small[:, member * width_small:(member + 1) * width_small]
        part_large = attn_large[:, member * width_large:(member + 1) * width_large]
        partial_value = jnp.dot(part_small, project_small[member * width_small:(member + 1) * width_small], preferred_element_type=jnp.float32)
        partial_value = partial_value + jnp.dot(part_large, project_large[member * width_large:(member + 1) * width_large], preferred_element_type=jnp.float32)
        projected = projected + lax.optimization_barrier(partial_value.astype(jnp.bfloat16)).astype(jnp.float32)
    resid = residual_in.astype(jnp.float32) + projected
    scale = lax.rsqrt(lax.optimization_barrier(jnp.mean(resid * resid, axis=1, keepdims=True)) + 1e-06)
    normed = (resid * scale * norm_gain.astype(jnp.float32)).astype(jnp.bfloat16)
    flat_route = routing.reshape(-1)
    flat_weight = route_weight.reshape(-1)
    per_expert = SEQUENCE_TOKENS // ROWS * CAP

    def one_expert(running, inputs):
        expert_id, weight_gate, weight_up, weight_down = inputs
        matches = flat_route == expert_id
        chosen = jnp.nonzero(matches, size=per_expert, fill_value=0)[0].astype(jnp.int32)
        valid = jnp.arange(per_expert) < jnp.sum(matches.astype(jnp.int32))
        token_ids = (chosen // TOP).astype(jnp.int32)
        rows_in = normed[token_ids]
        gate_part = jnp.dot(rows_in, weight_gate, preferred_element_type=jnp.float32)
        up_part = jnp.dot(rows_in, weight_up, preferred_element_type=jnp.float32)
        hidden = (jax.nn.silu(gate_part) * up_part).astype(jnp.bfloat16)
        result = jnp.dot(hidden, weight_down, preferred_element_type=jnp.float32).astype(jnp.bfloat16)
        factor = jnp.where(valid, flat_weight[chosen], jnp.zeros((), flat_weight.dtype))
        update = lax.optimization_barrier(result).astype(jnp.float32) * factor[:, None]
        return (running.at[token_ids].add(update), None)
    moe_sum, _ = lax.scan(one_expert, jnp.zeros((SEQUENCE_TOKENS, D), jnp.float32), (jnp.arange(EXPERTS, dtype=jnp.int32), expert_gate, expert_up, expert_down))
    return (resid + moe_sum).astype(jnp.bfloat16)
```

```python
import math

import jax
import jax.numpy as jnp
from jax import lax
from jax.experimental import pallas as pl
from jax.experimental.pallas import tpu as pltpu
from jax.sharding import PartitionSpec as P

BF = jnp.bfloat16
F32 = jnp.float32
LOG2E = math.log2(math.e)
GATE_ROWS = 16
PIECES = 3


def round16(n):
    return -(-n // 16) * 16


def in_pieces(gates, size):
    left = gates * -(size**0.5)
    rows = []
    for _ in range(PIECES):
        piece = lax.reduce_precision(left, 8, 7)
        rows.append(piece.astype(BF))
        left = left - piece
    stacked = jnp.concatenate(rows, axis=0)
    pad = GATE_ROWS - stacked.shape[0]
    return jnp.concatenate([stacked, jnp.zeros((pad, gates.shape[1]), BF)], axis=0)


def with_selector(queries, heads, size):
    tokens = queries.shape[0]
    per_head = queries.reshape(tokens, heads, size).transpose(1, 0, 2)
    column = jnp.arange(GATE_ROWS)[None, :]
    head = jnp.arange(heads)[:, None]
    chosen = (column % heads == head) & (column < PIECES * heads)
    chosen = jnp.broadcast_to(chosen.astype(BF)[:, None, :], (heads, tokens, GATE_ROWS))
    return jnp.concatenate([per_head, chosen], axis=2)


def attention_body(info, qs, ql, kv, gates, ps, pb, out, m_s, a_s, m_l, t_l, a_l):
    step = pl.program_id(0)
    heads_s, tokens, width_s = qs.shape
    heads_l, _, width_l = ql.shape
    ds, dl = width_s - GATE_ROWS, width_l - GATE_ROWS
    per_step = kv.shape[0]
    keys = per_step * kv.shape[2]
    sp = info[0]
    last = sp // per_step

    @pl.when(step == 0)
    def _():
        m_s[...] = jnp.full_like(m_s, -1e30)
        m_l[...] = jnp.full_like(m_l, -1e30)
        a_s[...] = jnp.zeros_like(a_s)
        a_l[...] = jnp.zeros_like(a_l)
        t_l[...] = jnp.zeros_like(t_l)

    def block(masked):
        def rows_of(ref, first, count):
            return jnp.concatenate([ref[i, first : first + count] for i in range(per_step)], axis=1)

        k_s = jnp.concatenate([rows_of(kv, 0, ds), rows_of(gates, 0, GATE_ROWS)], axis=0)
        v_s = rows_of(kv, ds, ds)
        k_l = jnp.concatenate([rows_of(kv, 2 * ds, dl), rows_of(gates, GATE_ROWS, GATE_ROWS)], axis=0)
        v_l = rows_of(kv, 2 * ds + dl, dl)
        ones = jnp.ones((GATE_ROWS, keys), BF)
        v_s = jnp.concatenate([v_s, ones], axis=0)
        if masked:
            q_pos = lax.broadcasted_iota(jnp.int32, (tokens, keys), 0) + (sp * tokens - step * keys)
            keep = q_pos >= lax.broadcasted_iota(jnp.int32, (tokens, keys), 1)

        def one(q, k, size, m_ref, h):
            s = jnp.dot(q[h], k, preferred_element_type=F32)
            if masked:
                s = jnp.where(keep, s, -1e30)
            top = m_ref[h]
            new = jnp.maximum(top, jnp.max(s, axis=1, keepdims=True))
            m_ref[h] = new
            c = LOG2E * size**-0.5
            return jnp.exp2((s - new) * c), jnp.exp2((top - new) * c)

        for h in range(heads_s):
            p, alpha = one(qs, k_s, ds, m_s, h)
            mixed = lax.dot_general(p.astype(BF), v_s, (((1,), (1,)), ((), ())), preferred_element_type=F32)
            a_s[h] = a_s[h] * alpha + mixed
        for h in range(heads_l):
            p, alpha = one(ql, k_l, dl, m_l, h)
            mixed = lax.dot_general(p.astype(BF), v_l, (((1,), (1,)), ((), ())), preferred_element_type=F32)
            a_l[h] = a_l[h] * alpha + mixed
            t_l[h] = t_l[h] * alpha + jnp.sum(p, axis=1, keepdims=True)

    @pl.when(step < last)
    def _():
        block(False)

    @pl.when(step == last)
    def _():
        block(True)

    @pl.when(step == pl.num_programs(0) - 1)
    def _():
        small = [(a_s[h, :, :ds] / a_s[h, :, ds : ds + 1]).astype(BF) for h in range(heads_s)]
        large = [(a_l[h] / t_l[h]).astype(BF) for h in range(heads_l)]
        total = jnp.dot(jnp.concatenate(small, axis=1), ps[...], preferred_element_type=F32)
        total = total + jnp.dot(jnp.concatenate(large, axis=1), pb[...], preferred_element_type=F32)
        out[...] = total.astype(BF)


def attention(info, qs, ql, kv, gates, ps, pb, per_step=4):
    blocks, _, block_keys = kv.shape
    tokens, width = qs.shape[1], ps.shape[1]
    ds, dl = qs.shape[2] - GATE_ROWS, ql.shape[2] - GATE_ROWS
    step_map = lambda j, i: (jnp.minimum(j, i[0] // per_step), 0, 0)
    whole = lambda a: pl.BlockSpec(a.shape, lambda j, i: (0,) * a.ndim)
    return pl.pallas_call(
        attention_body,
        grid_spec=pltpu.PrefetchScalarGridSpec(
            num_scalar_prefetch=1,
            grid=(blocks // per_step,),
            in_specs=[
                whole(qs),
                whole(ql),
                pl.BlockSpec((per_step,) + kv.shape[1:], step_map),
                pl.BlockSpec((per_step,) + gates.shape[1:], step_map),
                whole(ps),
                whole(pb),
            ],
            out_specs=pl.BlockSpec((tokens, width), lambda j, i: (0, 0)),
            scratch_shapes=[
                pltpu.VMEM((qs.shape[0], tokens, 1), F32),
                pltpu.VMEM((qs.shape[0], tokens, ds + GATE_ROWS), F32),
                pltpu.VMEM((ql.shape[0], tokens, 1), F32),
                pltpu.VMEM((ql.shape[0], tokens, 1), F32),
                pltpu.VMEM((ql.shape[0], tokens, dl), F32),
            ],
        ),
        out_shape=jax.ShapeDtypeStruct((tokens, width), BF),
        compiler_params=pltpu.CompilerParams(dimension_semantics=("arbitrary",), vmem_limit_bytes=60 << 20),
        name="attention",
    )(info, qs, ql, kv, gates, ps, pb)


def mix_body(parts, residual_in, gain, slots, resid_out, outgoing):
    projected = parts[0].astype(F32)
    for i in range(1, parts.shape[0]):
        projected = projected + parts[i].astype(F32)
    resid = residual_in[...].astype(F32) + projected
    resid_out[...] = resid
    scale = lax.rsqrt(jnp.mean(resid * resid, axis=1, keepdims=True) + 1e-06)
    normed = (resid * scale * gain[...].astype(F32)).astype(BF)
    outgoing[...] = jnp.dot(slots[...], normed, preferred_element_type=F32).astype(BF)


def mix(parts, residual_in, gain, slots):
    rows, width = residual_in.shape
    return pl.pallas_call(
        mix_body,
        out_shape=(
            jax.ShapeDtypeStruct((rows, width), F32),
            jax.ShapeDtypeStruct((slots.shape[0], width), BF),
        ),
        compiler_params=pltpu.CompilerParams(vmem_limit_bytes=40 << 20),
        name="mix",
    )(parts, residual_in, gain, slots)


def expert_body(rows, gate, up, down, out, total):
    step = pl.program_id(0)
    x = rows[...]
    g = jnp.dot(x, gate[0], preferred_element_type=F32)
    u = jnp.dot(x, up[0], preferred_element_type=F32)
    hidden = (g / (1.0 + jnp.exp(-g)) * u).astype(BF)
    part = jnp.dot(hidden, down[0], preferred_element_type=F32)

    @pl.when(step == 0)
    def _():
        total[...] = part

    @pl.when(step > 0)
    def _():
        total[...] += part

    @pl.when(step == pl.num_programs(0) - 1)
    def _():
        out[...] = total[...].astype(BF)


def expert(rows, gate, up, down, chunk=128):
    count, width = rows.shape
    units = gate.shape[2]
    return pl.pallas_call(
        expert_body,
        grid=(units // chunk,),
        in_specs=[
            pl.BlockSpec((count, width), lambda i: (0, 0)),
            pl.BlockSpec((1, width, chunk), lambda i: (0, 0, i)),
            pl.BlockSpec((1, width, chunk), lambda i: (0, 0, i)),
            pl.BlockSpec((1, chunk, width), lambda i: (0, i, 0)),
        ],
        out_specs=pl.BlockSpec((count, width), lambda i: (0, 0)),
        out_shape=jax.ShapeDtypeStruct((count, width), BF),
        scratch_shapes=[pltpu.VMEM((count, width), F32)],
        compiler_params=pltpu.CompilerParams(dimension_semantics=("arbitrary",), vmem_limit_bytes=40 << 20),
        name="expert",
    )(rows, gate, up, down)


def collect_body(returned, weights, resid, out):
    total = resid[...]
    for i in range(weights.shape[0]):
        total = total + jnp.dot(weights[i], returned[...], preferred_element_type=F32)
    out[...] = total.astype(BF)


def collect(returned, weights, resid):
    return pl.pallas_call(
        collect_body,
        out_shape=jax.ShapeDtypeStruct(resid.shape, BF),
        compiler_params=pltpu.CompilerParams(vmem_limit_bytes=40 << 20),
        name="collect",
    )(returned, weights, resid)


def three_pieces(value):
    pieces = []
    for _ in range(PIECES):
        piece = lax.reduce_precision(value, 8, 7)
        pieces.append(piece.astype(BF))
        value = value - piece
    return jnp.stack(pieces)


def shards(
    residual_in,
    query_small,
    query_large,
    key_small,
    key_large,
    value_small,
    value_large,
    forget_small,
    forget_large,
    project_small,
    project_large,
    norm_gain,
    expert_gate,
    expert_up,
    expert_down,
    routing,
    route_weight,
):
    head_devices = lax.axis_size("tp")
    experts = lax.axis_size("sp") * head_devices
    size_small, size_large = key_small.shape[0], key_large.shape[0]
    own_rows, width = residual_in.shape
    top_count = routing.shape[1]

    gates = jnp.concatenate([in_pieces(forget_small, size_small), in_pieces(forget_large, size_large)], axis=0)
    packed = jnp.concatenate([key_small, value_small, key_large, value_large], axis=0)
    all_gates = lax.all_gather(gates, "sp", axis=0)
    all_kv = lax.all_gather(packed, "sp", axis=0)

    info = lax.axis_index("sp").astype(jnp.int32).reshape(1)
    partial = attention(
        info,
        with_selector(query_small, forget_small.shape[0], size_small),
        with_selector(query_large, forget_large.shape[0], size_large),
        all_kv,
        all_gates,
        project_small,
        project_large,
    )

    capacity = max(2, 2 * own_rows * top_count // experts)
    pairs = own_rows * top_count
    pair_expert = routing.reshape(-1)
    same = pair_expert[:, None] == pair_expert[None, :]
    before = jnp.arange(pairs)[:, None] > jnp.arange(pairs)[None, :]
    slot = jnp.sum((same & before).astype(jnp.int32), axis=1)
    target = (pair_expert * capacity + slot).reshape(own_rows, top_count)
    hit = target[:, :, None] == jnp.arange(experts * capacity)[None, None, :]
    slots = jnp.any(hit, axis=1).T.astype(BF)
    weights = three_pieces(jnp.sum(jnp.where(hit, route_weight[:, :, None], 0.0), axis=1))

    parts = partial.reshape(head_devices, own_rows, width)
    parts = lax.all_to_all(parts, "tp", split_axis=0, concat_axis=0, tiled=True)
    resid, outgoing = mix(parts, residual_in, norm_gain.reshape(1, width), slots)
    outgoing = outgoing.reshape(experts, capacity, width)
    arrived = lax.all_to_all(outgoing, ("sp", "tp"), split_axis=0, concat_axis=0, tiled=True)
    result = expert(arrived.reshape(-1, width), expert_gate, expert_up, expert_down)
    result = result.reshape(experts, capacity, width)
    returned = lax.all_to_all(result, ("sp", "tp"), split_axis=0, concat_axis=0, tiled=True)
    return collect(returned.reshape(-1, width), weights, resid)


def solution(mesh):
    in_specs = (
        P(("grp", "sp", "tp"), None),
        P(("grp", "sp"), "tp"),
        P(("grp", "sp"), "tp"),
        P(None, ("grp", "sp")),
        P(None, ("grp", "sp")),
        P(None, ("grp", "sp")),
        P(None, ("grp", "sp")),
        P("tp", ("grp", "sp")),
        P("tp", ("grp", "sp")),
        P("tp", None),
        P("tp", None),
        P(),
        P(("sp", "tp"), None, None),
        P(("sp", "tp"), None, None),
        P(("sp", "tp"), None, None),
        P(("grp", "sp", "tp"), None),
        P(("grp", "sp", "tp"), None),
    )
    out_specs = P(("grp", "sp", "tp"), None)
    return jax.shard_map(shards, mesh=mesh, in_specs=in_specs, out_specs=out_specs, check_vma=False)
```

```python
import math

import jax
import jax.numpy as jnp
from jax import lax
from jax.experimental import pallas as pl
from jax.experimental.pallas import tpu as pltpu
from jax.sharding import PartitionSpec as P


BF = jnp.bfloat16
F32 = jnp.float32
LOG2E = math.log2(math.e)
GATE_ROWS = 16
PIECES = 3
LOW = -1e30


def params(mib=48):
    return pltpu.CompilerParams(vmem_limit_bytes=mib << 20)


def pack_body(key_small, key_large, value_small, value_large, gate_small, gate_large, out, gs, gl, sems):
    size_s, size_l = key_small.shape[0], key_large.shape[0]
    at_l = size_s + GATE_ROWS
    at_v = at_l + size_l + GATE_ROWS
    copies = [
        pltpu.make_async_copy(src, dst, sems.at[i])
        for i, (src, dst) in enumerate(
            (
                (gate_small, gs),
                (gate_large, gl),
                (key_small, out.at[pl.ds(0, size_s)]),
                (key_large, out.at[pl.ds(at_l, size_l)]),
                (value_small, out.at[pl.ds(at_v, size_s)]),
                (value_large, out.at[pl.ds(at_v + size_s, size_l)]),
            )
        )
    ]
    for copy in copies:
        copy.start()

    def pieces(gates, size):
        left = gates[...] * -(size**0.5)
        rows = []
        for _ in range(PIECES):
            piece = left.astype(BF).astype(F32)
            rows.append(piece)
            left = left - piece
        used = PIECES * gates.shape[0]
        rows.append(jnp.zeros((GATE_ROWS - used, gates.shape[1]), F32))
        return jnp.concatenate(rows, axis=0).astype(BF)

    copies[0].wait()
    copies[1].wait()
    out[size_s:at_l] = pieces(gs, size_s)
    out[at_l + size_l : at_v] = pieces(gl, size_l)
    for copy in copies[2:]:
        copy.wait()


def pack(key_small, key_large, value_small, value_large, gate_small, gate_large):
    rows = 2 * (key_small.shape[0] + key_large.shape[0] + GATE_ROWS)
    return pl.pallas_call(
        pack_body,
        in_specs=[pl.BlockSpec(memory_space=pltpu.HBM)] * 6,
        out_specs=pl.BlockSpec(memory_space=pltpu.VMEM),
        out_shape=jax.ShapeDtypeStruct((rows, key_small.shape[1]), BF),
        scratch_shapes=[
            pltpu.VMEM(gate_small.shape, F32),
            pltpu.VMEM(gate_large.shape, F32),
            pltpu.SemaphoreType.DMA((6,)),
        ],
        compiler_params=params(),
        name="pack",
    )(key_small, key_large, value_small, value_large, gate_small, gate_large)


def split_block(block, size_s, size_l):
    a = size_s + GATE_ROWS
    b = a + size_l + GATE_ROWS
    c = b + size_s
    spans = ((0, a), (b, c - b), (a, b - a), (c, size_l))
    return [block.at[pl.ds(start, count)] for start, count in spans]


def update(q, keys, values, state, h, size, keep=None):
    width = state.shape[2]
    edge = width * 3 // 4
    factor = LOG2E * size**-0.5
    old = state[h]
    s = jnp.concatenate([jnp.dot(q, k, preferred_element_type=F32) for k in keys], axis=1)
    if keep is not None:
        s = jnp.where(keep, s, LOW)
    top = old[:, edge : edge + 1]
    new = jnp.maximum(top, jnp.max(s, axis=1, keepdims=True))
    p = jnp.exp2((s - new) * factor).astype(BF)
    alpha = jnp.exp2((top - new) * factor)
    wide = jnp.concatenate(values, axis=1)
    count = wide.shape[1]
    wide = jnp.concatenate(
        [wide, jnp.ones((edge - size, count), BF), jnp.zeros((width - edge, count), BF)], axis=0
    )
    mixed = lax.dot_general(p, wide, (((1,), (1,)), ((), ())), preferred_element_type=F32)
    lane = lax.broadcasted_iota(jnp.int32, old.shape, 1)
    state[h] = jnp.where(lane >= edge, new, old * alpha + mixed)


def add_blocks(sets, blocks, keep=None):
    size_s = sets[0][0].shape[2] - GATE_ROWS
    size_l = sets[0][1].shape[2] - GATE_ROWS
    cut = [split_block(b, size_s, size_l) for b in blocks]

    def small(h, carry):
        for qs, _, state, _ in sets:
            update(qs[h], [c[0][...] for c in cut], [c[1][...] for c in cut], state, h, size_s, keep)
        return carry

    def large(h, carry):
        for _, ql, _, state in sets:
            update(ql[h], [c[2][...] for c in cut], [c[3][...] for c in cut], state, h, size_l, keep)
        return carry

    lax.fori_loop(0, sets[0][2].shape[0], small, 0)
    lax.fori_loop(0, sets[0][3].shape[0], large, 0)


def first_body(info, own_s, own_l, peer_s, peer_l, block, qs_o, ql_o, qs_p, ql_p, ss_o, sl_o, ss_p, sl_p):
    tokens = own_s.shape[0]

    def spread(queries, out):
        heads, _, width = out.shape
        size = width - GATE_ROWS
        column = lax.broadcasted_iota(jnp.int32, (tokens, GATE_ROWS), 1)
        for h in range(heads):
            chosen = (column % heads == h) & (column < PIECES * heads)
            out[h, :, :size] = queries[:, h * size : (h + 1) * size]
            out[h, :, size:] = jnp.where(chosen, 1.0, 0.0).astype(BF)

    spread(own_s, qs_o)
    spread(own_l, ql_o)
    spread(peer_s, qs_p)
    spread(peer_l, ql_p)
    for state in (ss_o, sl_o, ss_p, sl_p):
        lane = lax.broadcasted_iota(jnp.int32, state.shape, 2)
        state[...] = jnp.where(lane >= state.shape[2] * 3 // 4, LOW, 0.0)
    shape = (tokens, block.shape[1])
    keep = lax.broadcasted_iota(jnp.int32, shape, 0) >= lax.broadcasted_iota(jnp.int32, shape, 1)
    add_blocks([(qs_o, ql_o, ss_o, sl_o)], [block], keep)

    @pl.when(info[0] == 1)
    def _():
        add_blocks([(qs_p, ql_p, ss_p, sl_p)], [block])


def first(info, own_s, own_l, peer_s, peer_l, block, heads_s, heads_l):
    tokens = own_s.shape[0]
    size_s, size_l = own_s.shape[1] // heads_s, own_l.shape[1] // heads_l
    vm = pl.BlockSpec(memory_space=pltpu.VMEM)
    queries = [
        jax.ShapeDtypeStruct((heads_s, tokens, size_s + GATE_ROWS), BF),
        jax.ShapeDtypeStruct((heads_l, tokens, size_l + GATE_ROWS), BF),
    ]
    states = [
        jax.ShapeDtypeStruct((heads_s, tokens, 2 * size_s), F32),
        jax.ShapeDtypeStruct((heads_l, tokens, 2 * size_l), F32),
    ]
    return pl.pallas_call(
        first_body,
        in_specs=[pl.BlockSpec(memory_space=pltpu.SMEM)] + [vm] * 5,
        out_specs=[vm] * 8,
        out_shape=queries * 2 + states * 2,
        compiler_params=params(),
        name="first",
    )(info, own_s, own_l, peer_s, peer_l, block)


def advance(info, step, queries, blocks, states):
    def body(flags, qs_o, ql_o, qs_p, ql_p, *refs):
        arrived, (ss_o, sl_o, ss_p, sl_p) = refs[: len(blocks)], refs[-4:]

        @pl.when(flags[step] == 1)
        def _():
            add_blocks([(qs_o, ql_o, ss_o, sl_o), (qs_p, ql_p, ss_p, sl_p)], arrived)

    vm = pl.BlockSpec(memory_space=pltpu.VMEM)
    at = 1 + len(queries) + len(blocks)
    return pl.pallas_call(
        body,
        in_specs=[pl.BlockSpec(memory_space=pltpu.SMEM)] + [vm] * (at - 1 + len(states)),
        out_specs=[vm] * len(states),
        out_shape=[jax.ShapeDtypeStruct(s.shape, s.dtype) for s in states],
        input_output_aliases={at + i: i for i in range(len(states))},
        compiler_params=params(),
    )(info, *queries, *blocks, *states)


def finish_body(own_s, own_l, got_s, got_l, project_s, project_l, out):
    def attended(own, got):
        heads, _, width = own.shape
        size, edge = width // 2, width * 3 // 4
        factor = LOG2E * size**-0.5
        done = []
        for h in range(heads):
            a, b = own[h], got[h]
            top = jnp.maximum(a[:, edge : edge + 1], b[:, edge : edge + 1])
            wa = jnp.exp2((a[:, edge : edge + 1] - top) * factor)
            wb = jnp.exp2((b[:, edge : edge + 1] - top) * factor)
            both = a * wa + b * wb
            done.append((both[:, :size] / both[:, size : size + 1]).astype(BF))
        return jnp.concatenate(done, axis=1)

    total = jnp.dot(attended(own_s, got_s), project_s[...], preferred_element_type=F32)
    total = total + jnp.dot(attended(own_l, got_l), project_l[...], preferred_element_type=F32)
    out[...] = total.astype(BF)


def finish(own_s, own_l, got_s, got_l, project_s, project_l):
    return pl.pallas_call(
        finish_body,
        out_shape=jax.ShapeDtypeStruct((own_s.shape[1], project_s.shape[1]), BF),
        compiler_params=params(),
        name="finish",
    )(own_s, own_l, got_s, got_l, project_s, project_l)


def attend_and_project(qs, ql, key_small, key_large, value_small, value_large, gs, gl, ps, pb):
    devices = lax.axis_size("sp")
    chips = devices // 2
    place = lax.axis_index("sp").astype(jnp.int32)
    chip, core = place // 2, place % 2
    swap = [(i, i ^ 1) for i in range(devices)]
    ring = [(i, (i + 2 - 4 * (i % 2)) % devices) for i in range(devices)]
    steps = chips // 2
    k = jnp.arange(1, steps + 1, dtype=jnp.int32)
    usable = jnp.where(core == 0, chip >= k, chip + k >= chips).astype(jnp.int32)
    info = jnp.concatenate([(1 - core).reshape(1), usable])

    peer_s = lax.ppermute(qs, "sp", swap)
    peer_l = lax.ppermute(ql, "sp", swap)
    block = pack(key_small, key_large, value_small, value_large, gs, gl)
    b = lax.ppermute(block, "sp", swap)
    a = block
    made = first(info, qs, ql, peer_s, peer_l, block, gs.shape[0], gl.shape[0])
    queries, states = made[:4], made[4:]
    for step in range(1, steps + 1):
        a = lax.ppermute(a, "sp", ring)
        blocks = [a]
        if step < steps or chips % 2:
            b = lax.ppermute(b, "sp", ring)
            blocks.append(b)
        states = advance(info, step, queries, blocks, states)
    got_s = lax.ppermute(states[2], "sp", swap)
    got_l = lax.ppermute(states[3], "sp", swap)
    return finish(states[0], states[1], got_s, got_l, ps, pb)


def mix_body(parts, residual_in, gain, slots, resid_out, outgoing):
    projected = parts[0].astype(F32)
    for i in range(1, parts.shape[0]):
        projected = projected + parts[i].astype(F32)
    resid = residual_in[...].astype(F32) + projected
    resid_out[...] = resid
    scale = lax.rsqrt(jnp.mean(resid * resid, axis=1, keepdims=True) + 1e-06)
    normed = (resid * scale * gain[...].astype(F32)).astype(BF)
    outgoing[...] = jnp.dot(slots[...], normed, preferred_element_type=F32).astype(BF)


def mix(parts, residual_in, gain, slots):
    rows, width = residual_in.shape
    return pl.pallas_call(
        mix_body,
        out_shape=(
            jax.ShapeDtypeStruct((rows, width), F32),
            jax.ShapeDtypeStruct((slots.shape[0], width), BF),
        ),
        compiler_params=pltpu.CompilerParams(vmem_limit_bytes=40 << 20),
        name="mix",
    )(parts, residual_in, gain, slots)


def expert_body(rows, gate, up, down, out, total):
    step = pl.program_id(0)
    x = rows[...]
    g = jnp.dot(x, gate[0], preferred_element_type=F32)
    u = jnp.dot(x, up[0], preferred_element_type=F32)
    hidden = (g / (1.0 + jnp.exp(-g)) * u).astype(BF)
    part = jnp.dot(hidden, down[0], preferred_element_type=F32)

    @pl.when(step == 0)
    def _():
        total[...] = part

    @pl.when(step > 0)
    def _():
        total[...] += part

    @pl.when(step == pl.num_programs(0) - 1)
    def _():
        out[...] = total[...].astype(BF)


def expert(rows, gate, up, down, chunk=128):
    count, width = rows.shape
    units = gate.shape[2]
    return pl.pallas_call(
        expert_body,
        grid=(units // chunk,),
        in_specs=[
            pl.BlockSpec((count, width), lambda i: (0, 0)),
            pl.BlockSpec((1, width, chunk), lambda i: (0, 0, i)),
            pl.BlockSpec((1, width, chunk), lambda i: (0, 0, i)),
            pl.BlockSpec((1, chunk, width), lambda i: (0, i, 0)),
        ],
        out_specs=pl.BlockSpec((count, width), lambda i: (0, 0)),
        out_shape=jax.ShapeDtypeStruct((count, width), BF),
        scratch_shapes=[pltpu.VMEM((count, width), F32)],
        compiler_params=pltpu.CompilerParams(dimension_semantics=("arbitrary",), vmem_limit_bytes=40 << 20),
        name="expert",
    )(rows, gate, up, down)


def collect_body(returned, weights, resid, out):
    total = resid[...]
    for i in range(weights.shape[0]):
        total = total + jnp.dot(weights[i], returned[...], preferred_element_type=F32)
    out[...] = total.astype(BF)


def collect(returned, weights, resid):
    return pl.pallas_call(
        collect_body,
        out_shape=jax.ShapeDtypeStruct(resid.shape, BF),
        compiler_params=pltpu.CompilerParams(vmem_limit_bytes=40 << 20),
        name="collect",
    )(returned, weights, resid)


def three_pieces(value):
    pieces = []
    for _ in range(PIECES):
        piece = lax.reduce_precision(value, 8, 7)
        pieces.append(piece.astype(BF))
        value = value - piece
    return jnp.stack(pieces)


def shards(
    residual_in,
    query_small,
    query_large,
    key_small,
    key_large,
    value_small,
    value_large,
    forget_small,
    forget_large,
    project_small,
    project_large,
    norm_gain,
    expert_gate,
    expert_up,
    expert_down,
    routing,
    route_weight,
):
    head_devices = lax.axis_size("tp")
    experts = lax.axis_size("sp") * head_devices
    own_rows, width = residual_in.shape
    top_count = routing.shape[1]

    partial = attend_and_project(
        query_small,
        query_large,
        key_small,
        key_large,
        value_small,
        value_large,
        forget_small,
        forget_large,
        project_small,
        project_large,
    )

    capacity = max(2, 2 * own_rows * top_count // experts)
    pairs = own_rows * top_count
    pair_expert = routing.reshape(-1)
    same = pair_expert[:, None] == pair_expert[None, :]
    before = jnp.arange(pairs)[:, None] > jnp.arange(pairs)[None, :]
    slot = jnp.sum((same & before).astype(jnp.int32), axis=1)
    target = (pair_expert * capacity + slot).reshape(own_rows, top_count)
    hit = target[:, :, None] == jnp.arange(experts * capacity)[None, None, :]
    slots = jnp.any(hit, axis=1).T.astype(BF)
    weights = three_pieces(jnp.sum(jnp.where(hit, route_weight[:, :, None], 0.0), axis=1))

    parts = partial.reshape(head_devices, own_rows, width)
    parts = lax.all_to_all(parts, "tp", split_axis=0, concat_axis=0, tiled=True)
    resid, outgoing = mix(parts, residual_in, norm_gain.reshape(1, width), slots)
    outgoing = outgoing.reshape(experts, capacity, width)
    arrived = lax.all_to_all(outgoing, ("sp", "tp"), split_axis=0, concat_axis=0, tiled=True)
    result = expert(arrived.reshape(-1, width), expert_gate, expert_up, expert_down)
    result = result.reshape(experts, capacity, width)
    returned = lax.all_to_all(result, ("sp", "tp"), split_axis=0, concat_axis=0, tiled=True)
    return collect(returned.reshape(-1, width), weights, resid)


def solution(mesh):
    in_specs = (
        P(("grp", "sp", "tp"), None),
        P(("grp", "sp"), "tp"),
        P(("grp", "sp"), "tp"),
        P(None, ("grp", "sp")),
        P(None, ("grp", "sp")),
        P(None, ("grp", "sp")),
        P(None, ("grp", "sp")),
        P("tp", ("grp", "sp")),
        P("tp", ("grp", "sp")),
        P("tp", None),
        P("tp", None),
        P(),
        P(("sp", "tp"), None, None),
        P(("sp", "tp"), None, None),
        P(("sp", "tp"), None, None),
        P(("grp", "sp", "tp"), None),
        P(("grp", "sp", "tp"), None),
    )
    out_specs = P(("grp", "sp", "tp"), None)

    return jax.shard_map(shards, mesh=mesh, in_specs=in_specs, out_specs=out_specs, check_vma=False)
```

```python
import math

import jax
import jax.numpy as jnp
from jax import lax
from jax.experimental import pallas as pl
from jax.experimental.pallas import tpu as pltpu
from jax.sharding import PartitionSpec as P


BF = jnp.bfloat16
F32 = jnp.float32
LOG2E = math.log2(math.e)
GATE_ROWS = 16
PIECES = 3
LOW = -1e30


def params(mib=16):
    return pltpu.CompilerParams(vmem_limit_bytes=mib << 20)


def packed(keys_values, gates, size_s, size_l, heads_s):
    at_l = size_s + GATE_ROWS
    at_v = at_l + size_l + GATE_ROWS

    def body(kv, gate, out):
        def pieces(left, size):
            left = left * -(size**0.5)
            rows = []
            for _ in range(PIECES):
                piece = left.astype(BF).astype(F32)
                rows.append(piece)
                left = left - piece
            used = PIECES * left.shape[0]
            rows.append(jnp.zeros((GATE_ROWS - used, left.shape[1]), F32))
            return jnp.concatenate(rows, axis=0).astype(BF)

        out[:size_s] = kv[:size_s]
        out[size_s:at_l] = pieces(gate[:heads_s], size_s)
        out[at_l : at_l + size_l] = kv[size_s : size_s + size_l]
        out[at_l + size_l : at_v] = pieces(gate[heads_s:], size_l)
        out[at_v:] = kv[size_s + size_l :]

    return pl.pallas_call(
        body,
        out_shape=jax.ShapeDtypeStruct((at_v + size_s + size_l, keys_values.shape[1]), BF),
        compiler_params=params(),
        name="packed",
    )(keys_values, gates)


def update(units, keys, values, size, keep=None):
    factor = LOG2E * size**-0.5
    rows = size + GATE_ROWS
    tops = [state[h, rows : rows + 1] for _, state, h in units]

    def scores(i):
        q, _, h = units[i]
        s = jnp.dot(keys[...], q[h], preferred_element_type=F32)
        return s if keep is None else jnp.where(keep, s, LOW)

    s = scores(0)
    for i, (_, state, h) in enumerate(units):
        following = scores(i + 1) if i + 1 < len(units) else None
        new = jnp.maximum(tops[i], jnp.max(s, axis=0, keepdims=True))
        p = jnp.exp2((s - new) * factor).astype(BF)
        alpha = jnp.exp2((tops[i] - new) * factor)
        mixed = jnp.dot(values[...], p, preferred_element_type=F32)
        state[h, :rows] = state[h, :rows] * alpha + mixed
        state[h, rows:] = jnp.broadcast_to(new, (state.shape[1] - rows, new.shape[1]))
        s = following


def lay_out(blocks, ks, vs, kl, vl):
    size_s, size_l = ks.shape[1] - GATE_ROWS, kl.shape[1] - GATE_ROWS
    a = size_s + GATE_ROWS
    b = a + size_l + GATE_ROWS
    for i, block in enumerate(blocks):
        count = block.shape[1]
        at = pl.ds(i * count, count)
        ks[at] = block[0:a].T
        kl[at] = block[a:b].T
        vs[:size_s, at] = block[b : b + size_s]
        vl[:size_l, at] = block[b + size_s :]
    vs[size_s:] = jnp.ones((GATE_ROWS, vs.shape[1]), BF)
    vl[size_l:] = jnp.ones((GATE_ROWS, vl.shape[1]), BF)


def add_keys(sets, ks, vs, kl, vl, keep=None, together=1):
    def heads(which, keys, values):
        size = keys.shape[1] - GATE_ROWS
        count = sets[0][which].shape[0]
        group = math.gcd(together, count)

        def some(i, carry):
            units = [(one[which], one[which + 2], i * group + k) for k in range(group) for one in sets]
            update(units, keys, values, size, keep)
            return carry

        if count == group:
            some(0, 0)
        else:
            lax.fori_loop(0, count // group, some, 0)

    heads(0, ks, vs)
    heads(1, kl, vl)


def key_scratch(size_s, size_l, count):
    return [
        pltpu.VMEM((count, size_s + GATE_ROWS), BF),
        pltpu.VMEM((size_s + GATE_ROWS, count), BF),
        pltpu.VMEM((count, size_l + GATE_ROWS), BF),
        pltpu.VMEM((size_l + GATE_ROWS, count), BF),
    ]


def first_body(info, own_s, own_l, peer_s, peer_l, block, qs_o, ql_o, qs_p, ql_p, ss_o, sl_o, ss_p, sl_p, *laid):
    tokens = own_s.shape[0]

    def spread(queries, out):
        heads, width, _ = out.shape
        size = width - GATE_ROWS
        turned = queries[...].T
        row = lax.broadcasted_iota(jnp.int32, (GATE_ROWS, tokens), 0)
        for h in range(heads):
            chosen = (row % heads == h) & (row < PIECES * heads)
            out[h, :size] = turned[h * size : (h + 1) * size]
            out[h, size:] = jnp.where(chosen, 1.0, 0.0).astype(BF)

    lay_out([block], *laid)
    spread(own_s, qs_o)
    spread(own_l, ql_o)
    spread(peer_s, qs_p)
    spread(peer_l, ql_p)
    for state in (ss_o, sl_o, ss_p, sl_p):
        heads, rows, _ = state.shape
        state[:, : rows - 8] = jnp.zeros((heads, rows - 8, tokens), F32)
        state[:, rows - 8 :] = jnp.full((heads, 8, tokens), LOW, F32)
    shape = (block.shape[1], tokens)
    keep = lax.broadcasted_iota(jnp.int32, shape, 1) >= lax.broadcasted_iota(jnp.int32, shape, 0)
    add_keys([(qs_o, ql_o, ss_o, sl_o)], *laid, keep=keep)

    @pl.when(info[0] == 1)
    def _():
        add_keys([(qs_p, ql_p, ss_p, sl_p)], *laid)


def first(info, own_s, own_l, peer_s, peer_l, block, heads_s, heads_l):
    tokens = own_s.shape[0]
    size_s, size_l = own_s.shape[1] // heads_s, own_l.shape[1] // heads_l
    vm = pl.BlockSpec(memory_space=pltpu.VMEM)
    queries = [
        jax.ShapeDtypeStruct((heads_s, size_s + GATE_ROWS, tokens), BF),
        jax.ShapeDtypeStruct((heads_l, size_l + GATE_ROWS, tokens), BF),
    ]
    states = [
        jax.ShapeDtypeStruct((heads_s, size_s + GATE_ROWS + 8, tokens), F32),
        jax.ShapeDtypeStruct((heads_l, size_l + GATE_ROWS + 8, tokens), F32),
    ]
    return pl.pallas_call(
        first_body,
        in_specs=[pl.BlockSpec(memory_space=pltpu.SMEM)] + [vm] * 5,
        out_specs=[vm] * 8,
        out_shape=queries * 2 + states * 2,
        scratch_shapes=key_scratch(size_s, size_l, block.shape[1]),
        compiler_params=params(),
        name="first",
    )(info, own_s, own_l, peer_s, peer_l, block)


def advance(info, step, queries, blocks, states):
    def body(flags, qs_o, ql_o, qs_p, ql_p, *refs):
        arrived, (ss_o, sl_o, ss_p, sl_p), laid = refs[: len(blocks)], refs[-8:-4], refs[-4:]

        @pl.when(flags[step] == 1)
        def _():
            lay_out(arrived, *laid)
            add_keys([(qs_o, ql_o, ss_o, sl_o), (qs_p, ql_p, ss_p, sl_p)], *laid)

    vm = pl.BlockSpec(memory_space=pltpu.VMEM)
    at = 1 + len(queries) + len(blocks)
    size_s, size_l = queries[0].shape[1] - GATE_ROWS, queries[1].shape[1] - GATE_ROWS
    return pl.pallas_call(
        body,
        in_specs=[pl.BlockSpec(memory_space=pltpu.SMEM)] + [vm] * (at - 1 + len(states)),
        out_specs=[vm] * len(states),
        out_shape=[jax.ShapeDtypeStruct(s.shape, s.dtype) for s in states],
        input_output_aliases={at + i: i for i in range(len(states))},
        scratch_shapes=key_scratch(size_s, size_l, sum(b.shape[1] for b in blocks)),
        compiler_params=params(),
    )(info, *queries, *blocks, *states)


def finish_body(own_s, own_l, got_s, got_l, project_s, project_l, out):
    def attended(own, got):
        heads, rows, _ = own.shape
        size = rows - 8 - GATE_ROWS
        factor = LOG2E * size**-0.5
        done = []
        for h in range(heads):
            a, b = own[h, rows - 8 : rows - 7], got[h, rows - 8 : rows - 7]
            top = jnp.maximum(a, b)
            wa, wb = jnp.exp2((a - top) * factor), jnp.exp2((b - top) * factor)
            total = own[h, size : size + 1] * wa + got[h, size : size + 1] * wb
            sums = own[h, :size] * wa + got[h, :size] * wb
            done.append((sums / total).astype(BF))
        return jnp.concatenate(done, axis=0).T

    total = jnp.dot(attended(own_s, got_s), project_s[...], preferred_element_type=F32)
    total = total + jnp.dot(attended(own_l, got_l), project_l[...], preferred_element_type=F32)
    out[...] = total.astype(BF)


def finish(own_s, own_l, got_s, got_l, project_s, project_l):
    return pl.pallas_call(
        finish_body,
        out_shape=jax.ShapeDtypeStruct((own_s.shape[2], project_s.shape[1]), BF),
        compiler_params=params(),
        name="finish",
    )(own_s, own_l, got_s, got_l, project_s, project_l)


def attend_and_project(qs, ql, key_small, key_large, value_small, value_large, gs, gl, ps, pb):
    devices = lax.axis_size("sp")
    chips = devices // 2
    place = lax.axis_index("sp").astype(jnp.int32)
    chip, core = place // 2, place % 2
    swap = [(i, i ^ 1) for i in range(devices)]
    ring = [(i, (i + 2 - 4 * (i % 2)) % devices) for i in range(devices)]
    steps = chips // 2
    k = jnp.arange(1, steps + 1, dtype=jnp.int32)
    usable = jnp.where(core == 0, chip >= k, chip + k >= chips).astype(jnp.int32)
    info = jnp.concatenate([(1 - core).reshape(1), usable])

    peer_s = lax.ppermute(qs, "sp", swap)
    peer_l = lax.ppermute(ql, "sp", swap)
    kv = jnp.concatenate([key_small, key_large, value_small, value_large], axis=0)
    gates = jnp.concatenate([gs, gl], axis=0)
    block = packed(kv, gates, key_small.shape[0], key_large.shape[0], gs.shape[0])
    b = lax.ppermute(block, "sp", swap)
    a = block
    made = first(info, qs, ql, peer_s, peer_l, block, gs.shape[0], gl.shape[0])
    queries, states = made[:4], made[4:]
    for step in range(1, steps + 1):
        a = lax.ppermute(a, "sp", ring)
        blocks = [a]
        if step < steps or chips % 2:
            b = lax.ppermute(b, "sp", ring)
            blocks.append(b)
        states = advance(info, step, queries, blocks, states)
    got_s = lax.ppermute(states[2], "sp", swap)
    got_l = lax.ppermute(states[3], "sp", swap)
    return finish(states[0], states[1], got_s, got_l, ps, pb)


def mix_body(parts, residual_in, gain, slots, resid_out, outgoing):
    projected = parts[0].astype(F32)
    for i in range(1, parts.shape[0]):
        projected = projected + parts[i].astype(F32)
    resid = residual_in[...].astype(F32) + projected
    resid_out[...] = resid
    scale = lax.rsqrt(jnp.mean(resid * resid, axis=1, keepdims=True) + 1e-06)
    normed = (resid * scale * gain[...].astype(F32)).astype(BF)
    outgoing[...] = jnp.dot(slots[...], normed, preferred_element_type=F32).astype(BF)


def mix(parts, residual_in, gain, slots):
    rows, width = residual_in.shape
    return pl.pallas_call(
        mix_body,
        out_shape=(
            jax.ShapeDtypeStruct((rows, width), F32),
            jax.ShapeDtypeStruct((slots.shape[0], width), BF),
        ),
        compiler_params=params(),
        name="mix",
    )(parts, residual_in, gain, slots)


def expert_body(rows, gate, up, down, out, total):
    step = pl.program_id(0)
    g = jnp.dot(rows[...], gate[0], preferred_element_type=F32)
    u = jnp.dot(rows[...], up[0], preferred_element_type=F32)
    hidden = (g / (1.0 + jnp.exp(-g)) * u).astype(BF)
    width = out.shape[1]
    span = math.gcd(width, 512)
    final = pl.num_programs(0) - 1

    def piece(i, carry):
        at = pl.ds(pl.multiple_of(i * span, span), span)
        part = jnp.dot(hidden, down[0, :, at], preferred_element_type=F32)

        @pl.when(step == 0)
        def _():
            total[:, at] = part

        @pl.when((step > 0) & (step < final))
        def _():
            total[:, at] += part

        @pl.when(step == final)
        def _():
            out[:, at] = (total[:, at] + part).astype(BF)

        return carry

    lax.fori_loop(0, width // span, piece, 0)


def expert(rows, gate, up, down):
    count, width = rows.shape
    units = gate.shape[2]
    chunk = math.gcd(units // 2, 128)
    return pl.pallas_call(
        expert_body,
        grid=(units // chunk,),
        in_specs=[
            pl.BlockSpec((count, width), lambda i: (0, 0)),
            pl.BlockSpec((1, width, chunk), lambda i: (0, 0, i)),
            pl.BlockSpec((1, width, chunk), lambda i: (0, 0, i)),
            pl.BlockSpec((1, chunk, width), lambda i: (0, i, 0)),
        ],
        out_specs=pl.BlockSpec((count, width), lambda i: (0, 0)),
        out_shape=jax.ShapeDtypeStruct((count, width), BF),
        scratch_shapes=[pltpu.VMEM((count, width), F32)],
        compiler_params=params(60),
        name="expert",
    )(rows, gate, up, down)


def collect_body(returned, weights, resid, out):
    total = resid[...]
    for i in range(weights.shape[0]):
        total = total + jnp.dot(weights[i], returned[...], preferred_element_type=F32)
    out[...] = total.astype(BF)


def collect(returned, weights, resid):
    return pl.pallas_call(
        collect_body,
        out_shape=jax.ShapeDtypeStruct(resid.shape, BF),
        compiler_params=params(),
        name="collect",
    )(returned, weights, resid)


def three_pieces(value):
    pieces = []
    for _ in range(PIECES):
        piece = lax.reduce_precision(value, 8, 7)
        pieces.append(piece.astype(BF))
        value = value - piece
    return jnp.stack(pieces)


def shards(
    residual_in,
    query_small,
    query_large,
    key_small,
    key_large,
    value_small,
    value_large,
    forget_small,
    forget_large,
    project_small,
    project_large,
    norm_gain,
    expert_gate,
    expert_up,
    expert_down,
    routing,
    route_weight,
):
    head_devices = lax.axis_size("tp")
    experts = lax.axis_size("sp") * head_devices
    own_rows, width = residual_in.shape
    top_count = routing.shape[1]

    partial = attend_and_project(
        query_small,
        query_large,
        key_small,
        key_large,
        value_small,
        value_large,
        forget_small,
        forget_large,
        project_small,
        project_large,
    )

    capacity = max(2, 2 * own_rows * top_count // experts)
    pairs = own_rows * top_count
    pair_expert = routing.reshape(-1)
    same = pair_expert[:, None] == pair_expert[None, :]
    before = jnp.arange(pairs)[:, None] > jnp.arange(pairs)[None, :]
    slot = jnp.sum((same & before).astype(jnp.int32), axis=1)
    target = (pair_expert * capacity + slot).reshape(own_rows, top_count)
    hit = target[:, :, None] == jnp.arange(experts * capacity)[None, None, :]
    slots = jnp.any(hit, axis=1).T.astype(BF)
    weights = three_pieces(jnp.sum(jnp.where(hit, route_weight[:, :, None], 0.0), axis=1))

    parts = partial.reshape(head_devices, own_rows, width)
    parts = lax.all_to_all(parts, "tp", split_axis=0, concat_axis=0, tiled=True)
    resid, outgoing = mix(parts, residual_in, norm_gain.reshape(1, width), slots)
    outgoing = outgoing.reshape(experts, capacity, width)
    arrived = lax.all_to_all(outgoing, ("sp", "tp"), split_axis=0, concat_axis=0, tiled=True)
    result = expert(arrived.reshape(-1, width), expert_gate, expert_up, expert_down)
    result = result.reshape(experts, capacity, width)
    returned = lax.all_to_all(result, ("sp", "tp"), split_axis=0, concat_axis=0, tiled=True)
    return collect(returned.reshape(-1, width), weights, resid)


def solution(mesh):
    in_specs = (
        P(("grp", "sp", "tp"), None),
        P(("grp", "sp"), "tp"),
        P(("grp", "sp"), "tp"),
        P(None, ("grp", "sp")),
        P(None, ("grp", "sp")),
        P(None, ("grp", "sp")),
        P(None, ("grp", "sp")),
        P("tp", ("grp", "sp")),
        P("tp", ("grp", "sp")),
        P("tp", None),
        P("tp", None),
        P(),
        P(("sp", "tp"), None, None),
        P(("sp", "tp"), None, None),
        P(("sp", "tp"), None, None),
        P(("grp", "sp", "tp"), None),
        P(("grp", "sp", "tp"), None),
    )
    out_specs = P(("grp", "sp", "tp"), None)

    return jax.shard_map(shards, mesh=mesh, in_specs=in_specs, out_specs=out_specs, check_vma=False)
```

```python
import functools
import math

import jax
import jax.numpy as jnp
from jax import lax
from jax.experimental import pallas as pl
from jax.experimental.pallas import tpu as pltpu
from jax.sharding import PartitionSpec as P


BF = jnp.bfloat16
F32 = jnp.float32
LOG2E = math.log2(math.e)
GATE_ROWS = 16
PIECES = 3
LOW = -1e30


def params(mib=16):
    return pltpu.CompilerParams(vmem_limit_bytes=mib << 20)


def packed(keys_values, gates, size_s, size_l, heads_s):
    at_l = size_s + GATE_ROWS
    at_v = at_l + size_l + GATE_ROWS

    def body(kv, gate, out):
        def pieces(left, size):
            left = left * -(size**0.5)
            rows = []
            for _ in range(PIECES):
                piece = left.astype(BF).astype(F32)
                rows.append(piece)
                left = left - piece
            used = PIECES * left.shape[0]
            rows.append(jnp.zeros((GATE_ROWS - used, left.shape[1]), F32))
            return jnp.concatenate(rows, axis=0).astype(BF)

        out[:size_s] = kv[:size_s]
        out[size_s:at_l] = pieces(gate[:heads_s], size_s)
        out[at_l : at_l + size_l] = kv[size_s : size_s + size_l]
        out[at_l + size_l : at_v] = pieces(gate[heads_s:], size_l)
        out[at_v:] = kv[size_s + size_l :]

    return pl.pallas_call(
        body,
        out_shape=jax.ShapeDtypeStruct((at_v + size_s + size_l, keys_values.shape[1]), BF),
        compiler_params=params(),
        name="packed",
    )(keys_values, gates)


def update(units, keys, values, size, keep=None):
    factor = LOG2E * size**-0.5
    rows = size + GATE_ROWS
    tops = [state[h, rows : rows + 1] for _, state, h in units]

    def scores(i):
        q, _, h = units[i]
        s = jnp.dot(keys[...], q[h], preferred_element_type=F32)
        return s if keep is None else jnp.where(keep, s, LOW)

    s = scores(0)
    for i, (_, state, h) in enumerate(units):
        following = scores(i + 1) if i + 1 < len(units) else None
        new = jnp.maximum(tops[i], jnp.max(s, axis=0, keepdims=True))
        p = jnp.exp2((s - new) * factor).astype(BF)
        alpha = jnp.exp2((tops[i] - new) * factor)
        mixed = jnp.dot(values[...], p, preferred_element_type=F32)
        state[h, :rows] = state[h, :rows] * alpha + mixed
        state[h, rows:] = jnp.broadcast_to(new, (state.shape[1] - rows, new.shape[1]))
        s = following


def lay_out(blocks, ks, vs, kl, vl, usable=None):
    size_s, size_l = ks.shape[1] - GATE_ROWS, kl.shape[1] - GATE_ROWS
    a = size_s + GATE_ROWS
    b = a + size_l + GATE_ROWS
    for i, block in enumerate(blocks):
        count = block.shape[1]
        at = pl.ds(i * count, count)

        def with_gates(first, size):
            gates = block[first + size : first + size + GATE_ROWS]
            if usable is not None:
                gates = jnp.where(usable[i] == 1, gates.astype(F32), LOW).astype(BF)
            return jnp.concatenate([block[first : first + size], gates], axis=0).T

        ks[at] = with_gates(0, size_s)
        kl[at] = with_gates(a, size_l)
        vs[:size_s, at] = block[b : b + size_s]
        vl[:size_l, at] = block[b + size_s :]
    vs[size_s:] = jnp.ones((GATE_ROWS, vs.shape[1]), BF)
    vl[size_l:] = jnp.ones((GATE_ROWS, vl.shape[1]), BF)


def add_keys(sets, ks, vs, kl, vl, keep=None, together=1):
    def heads(which, keys, values):
        size = keys.shape[1] - GATE_ROWS
        count = sets[0][which].shape[0]
        group = math.gcd(together, count)

        def some(i, carry):
            units = [(one[which], one[which + 2], i * group + k) for k in range(group) for one in sets]
            update(units, keys, values, size, keep)
            return carry

        if count == group:
            some(0, 0)
        else:
            lax.fori_loop(0, count // group, some, 0)

    heads(0, ks, vs)
    heads(1, kl, vl)


def key_scratch(size_s, size_l, count):
    return [
        pltpu.VMEM((count, size_s + GATE_ROWS), BF),
        pltpu.VMEM((size_s + GATE_ROWS, count), BF),
        pltpu.VMEM((count, size_l + GATE_ROWS), BF),
        pltpu.VMEM((size_l + GATE_ROWS, count), BF),
    ]


def first_body(info, own_s, own_l, peer_s, peer_l, block, qs_o, ql_o, qs_p, ql_p, ss_o, sl_o, ss_p, sl_p, *laid):
    tokens = own_s.shape[0]

    def spread(queries, out):
        heads, width, _ = out.shape
        size = width - GATE_ROWS
        turned = queries[...].T
        row = lax.broadcasted_iota(jnp.int32, (GATE_ROWS, tokens), 0)
        for h in range(heads):
            chosen = (row % heads == h) & (row < PIECES * heads)
            out[h, :size] = turned[h * size : (h + 1) * size]
            out[h, size:] = jnp.where(chosen, 1.0, 0.0).astype(BF)

    lay_out([block], *laid)
    spread(own_s, qs_o)
    spread(own_l, ql_o)
    spread(peer_s, qs_p)
    spread(peer_l, ql_p)
    for state in (ss_o, sl_o, ss_p, sl_p):
        heads, rows, _ = state.shape
        state[:, : rows - 8] = jnp.zeros((heads, rows - 8, tokens), F32)
        state[:, rows - 8 :] = jnp.full((heads, 8, tokens), LOW, F32)
    shape = (block.shape[1], tokens)
    keep = lax.broadcasted_iota(jnp.int32, shape, 1) >= lax.broadcasted_iota(jnp.int32, shape, 0)
    add_keys([(qs_o, ql_o, ss_o, sl_o)], *laid, keep=keep)

    @pl.when(info[0] == 1)
    def _():
        add_keys([(qs_p, ql_p, ss_p, sl_p)], *laid)


def first(info, own_s, own_l, peer_s, peer_l, block, heads_s, heads_l):
    tokens = own_s.shape[0]
    size_s, size_l = own_s.shape[1] // heads_s, own_l.shape[1] // heads_l
    vm = pl.BlockSpec(memory_space=pltpu.VMEM)
    queries = [
        jax.ShapeDtypeStruct((heads_s, size_s + GATE_ROWS, tokens), BF),
        jax.ShapeDtypeStruct((heads_l, size_l + GATE_ROWS, tokens), BF),
    ]
    states = [
        jax.ShapeDtypeStruct((heads_s, size_s + GATE_ROWS + 8, tokens), F32),
        jax.ShapeDtypeStruct((heads_l, size_l + GATE_ROWS + 8, tokens), F32),
    ]
    return pl.pallas_call(
        first_body,
        in_specs=[pl.BlockSpec(memory_space=pltpu.SMEM)] + [vm] * 5,
        out_specs=[vm] * 8,
        out_shape=queries * 2 + states * 2,
        scratch_shapes=key_scratch(size_s, size_l, block.shape[1]),
        compiler_params=params(),
        name="first",
    )(info, own_s, own_l, peer_s, peer_l, block)


def advance(info, steps, queries, blocks, states):
    def body(flags, qs_o, ql_o, qs_p, ql_p, *refs):
        arrived, (ss_o, sl_o, ss_p, sl_p), laid = refs[: len(blocks)], refs[-8:-4], refs[-4:]
        usable = [flags[step] for step in steps]
        some = functools.reduce(jnp.maximum, usable)

        @pl.when(some == 1)
        def _():
            lay_out(arrived, *laid, usable=usable)
            add_keys([(qs_o, ql_o, ss_o, sl_o), (qs_p, ql_p, ss_p, sl_p)], *laid)

    vm = pl.BlockSpec(memory_space=pltpu.VMEM)
    at = 1 + len(queries) + len(blocks)
    size_s, size_l = queries[0].shape[1] - GATE_ROWS, queries[1].shape[1] - GATE_ROWS
    return pl.pallas_call(
        body,
        in_specs=[pl.BlockSpec(memory_space=pltpu.SMEM)] + [vm] * (at - 1 + len(states)),
        out_specs=[vm] * len(states),
        out_shape=[jax.ShapeDtypeStruct(s.shape, s.dtype) for s in states],
        input_output_aliases={at + i: i for i in range(len(states))},
        scratch_shapes=key_scratch(size_s, size_l, sum(b.shape[1] for b in blocks)),
        compiler_params=params(),
    )(info, *queries, *blocks, *states)


def finish_body(own_s, own_l, got_s, got_l, project_s, project_l, out):
    def attended(own, got):
        heads, rows, _ = own.shape
        size = rows - 8 - GATE_ROWS
        factor = LOG2E * size**-0.5
        done = []
        for h in range(heads):
            a, b = own[h, rows - 8 : rows - 7], got[h, rows - 8 : rows - 7]
            top = jnp.maximum(a, b)
            wa, wb = jnp.exp2((a - top) * factor), jnp.exp2((b - top) * factor)
            total = own[h, size : size + 1] * wa + got[h, size : size + 1] * wb
            sums = own[h, :size] * wa + got[h, :size] * wb
            done.append((sums / total).astype(BF))
        return jnp.concatenate(done, axis=0).T

    total = jnp.dot(attended(own_s, got_s), project_s[...], preferred_element_type=F32)
    total = total + jnp.dot(attended(own_l, got_l), project_l[...], preferred_element_type=F32)
    out[...] = total.astype(BF)


def finish(own_s, own_l, got_s, got_l, project_s, project_l):
    return pl.pallas_call(
        finish_body,
        out_shape=jax.ShapeDtypeStruct((own_s.shape[2], project_s.shape[1]), BF),
        compiler_params=params(),
        name="finish",
    )(own_s, own_l, got_s, got_l, project_s, project_l)


def attend_and_project(qs, ql, key_small, key_large, value_small, value_large, gs, gl, ps, pb):
    devices = lax.axis_size("sp")
    chips = devices // 2
    place = lax.axis_index("sp").astype(jnp.int32)
    chip, core = place // 2, place % 2
    swap = [(i, i ^ 1) for i in range(devices)]
    ring = [(i, (i + 2 - 4 * (i % 2)) % devices) for i in range(devices)]
    steps = chips // 2
    k = jnp.arange(1, steps + 1, dtype=jnp.int32)
    usable = jnp.where(core == 0, chip >= k, chip + k >= chips).astype(jnp.int32)
    info = jnp.concatenate([(1 - core).reshape(1), usable])

    peer_s = lax.ppermute(qs, "sp", swap)
    peer_l = lax.ppermute(ql, "sp", swap)
    kv = jnp.concatenate([key_small, key_large, value_small, value_large], axis=0)
    gates = jnp.concatenate([gs, gl], axis=0)
    block = packed(kv, gates, key_small.shape[0], key_large.shape[0], gs.shape[0])
    b = lax.ppermute(block, "sp", swap)
    a = block
    made = first(info, qs, ql, peer_s, peer_l, block, gs.shape[0], gl.shape[0])
    queries, states = made[:4], made[4:]
    waiting, at = [], []
    for step in range(1, steps + 1):
        a = lax.ppermute(a, "sp", ring)
        waiting.append(a)
        at.append(step)
        if step < steps or chips % 2:
            b = lax.ppermute(b, "sp", ring)
            waiting.append(b)
            at.append(step)
        if worked_at(step, steps):
            states = advance(info, at, queries, waiting, states)
            waiting, at = [], []
    got_s = lax.ppermute(states[2], "sp", swap)
    got_l = lax.ppermute(states[3], "sp", swap)
    return finish(states[0], states[1], got_s, got_l, ps, pb)


def worked_at(step, steps):
    return step % 2 == 1 or step == steps


def mix_body(parts, residual_in, gain, slots, resid_out, outgoing):
    projected = parts[0].astype(F32)
    for i in range(1, parts.shape[0]):
        projected = projected + parts[i].astype(F32)
    resid = residual_in[...].astype(F32) + projected
    resid_out[...] = resid
    scale = lax.rsqrt(jnp.mean(resid * resid, axis=1, keepdims=True) + 1e-06)
    normed = (resid * scale * gain[...].astype(F32)).astype(BF)
    outgoing[...] = jnp.dot(slots[...], normed, preferred_element_type=F32).astype(BF)


def mix(parts, residual_in, gain, slots):
    rows, width = residual_in.shape
    return pl.pallas_call(
        mix_body,
        out_shape=(
            jax.ShapeDtypeStruct((rows, width), F32),
            jax.ShapeDtypeStruct((slots.shape[0], width), BF),
        ),
        compiler_params=params(),
        name="mix",
    )(parts, residual_in, gain, slots)


def expert(rows, gate, up, down):
    count, width = rows.shape
    units = gate.shape[2]
    pieces = 4
    deep = width // pieces
    span = math.gcd(width, 512)

    def body(rows, gate, up, down, out, gate_v, up_v, down_v, g, u, hidden, sems):
        def inward(i):
            at = pl.ds(pl.multiple_of(i * deep, deep), deep)
            return (
                pltpu.make_async_copy(gate.at[0, at], gate_v.at[at], sems.at[2 * i]),
                pltpu.make_async_copy(up.at[0, at], up_v.at[at], sems.at[2 * i + 1]),
            )

        outward = pltpu.make_async_copy(down.at[0], down_v, sems.at[2 * pieces])
        for i in range(pieces):
            for copy in inward(i):
                copy.start()
        outward.start()
        g[...] = jnp.zeros_like(g)
        u[...] = jnp.zeros_like(u)

        def first_products(i, carry):
            at = pl.ds(pl.multiple_of(i * deep, deep), deep)
            for copy, weight, total in zip(inward(i), (gate_v, up_v), (g, u)):
                copy.wait()
                total[...] += jnp.dot(rows[:, at], weight[at], preferred_element_type=F32)
            return carry

        lax.fori_loop(0, pieces, first_products, 0)
        gated = g[...]
        hidden[...] = (gated / (1.0 + jnp.exp(-gated)) * u[...]).astype(BF)
        outward.wait()

        def last_product(i, carry):
            at = pl.ds(pl.multiple_of(i * span, span), span)
            out[:, at] = jnp.dot(hidden[...], down_v[:, at], preferred_element_type=F32).astype(BF)
            return carry

        lax.fori_loop(0, width // span, last_product, 0)

    vm = pl.BlockSpec(memory_space=pltpu.VMEM)
    return pl.pallas_call(
        body,
        in_specs=[vm] + [pl.BlockSpec(memory_space=pltpu.HBM)] * 3,
        out_specs=vm,
        out_shape=jax.ShapeDtypeStruct((count, width), BF),
        scratch_shapes=[
            pltpu.VMEM((width, units), BF),
            pltpu.VMEM((width, units), BF),
            pltpu.VMEM((units, width), BF),
            pltpu.VMEM((count, units), F32),
            pltpu.VMEM((count, units), F32),
            pltpu.VMEM((count, units), BF),
            pltpu.SemaphoreType.DMA((2 * pieces + 1,)),
        ],
        compiler_params=params(57),
        name="expert",
    )(rows, gate, up, down)


def collect_body(returned, weights, resid, out):
    total = resid[...]
    for i in range(weights.shape[0]):
        total = total + jnp.dot(weights[i], returned[...], preferred_element_type=F32)
    out[...] = total.astype(BF)


def collect(returned, weights, resid):
    return pl.pallas_call(
        collect_body,
        out_shape=jax.ShapeDtypeStruct(resid.shape, BF),
        compiler_params=params(),
        name="collect",
    )(returned, weights, resid)


def three_pieces(value):
    pieces = []
    for _ in range(PIECES):
        piece = lax.reduce_precision(value, 8, 7)
        pieces.append(piece.astype(BF))
        value = value - piece
    return jnp.stack(pieces)


def shards(
    residual_in,
    query_small,
    query_large,
    key_small,
    key_large,
    value_small,
    value_large,
    forget_small,
    forget_large,
    project_small,
    project_large,
    norm_gain,
    expert_gate,
    expert_up,
    expert_down,
    routing,
    route_weight,
):
    head_devices = lax.axis_size("tp")
    experts = lax.axis_size("sp") * head_devices
    own_rows, width = residual_in.shape
    top_count = routing.shape[1]

    partial = attend_and_project(
        query_small,
        query_large,
        key_small,
        key_large,
        value_small,
        value_large,
        forget_small,
        forget_large,
        project_small,
        project_large,
    )

    capacity = max(2, 2 * own_rows * top_count // experts)
    pairs = own_rows * top_count
    pair_expert = routing.reshape(-1)
    same = pair_expert[:, None] == pair_expert[None, :]
    before = jnp.arange(pairs)[:, None] > jnp.arange(pairs)[None, :]
    slot = jnp.sum((same & before).astype(jnp.int32), axis=1)
    target = (pair_expert * capacity + slot).reshape(own_rows, top_count)
    hit = target[:, :, None] == jnp.arange(experts * capacity)[None, None, :]
    slots = jnp.any(hit, axis=1).T.astype(BF)
    weights = three_pieces(jnp.sum(jnp.where(hit, route_weight[:, :, None], 0.0), axis=1))

    parts = partial.reshape(head_devices, own_rows, width)
    parts = lax.all_to_all(parts, "tp", split_axis=0, concat_axis=0, tiled=True)
    resid, outgoing = mix(parts, residual_in, norm_gain.reshape(1, width), slots)
    outgoing = outgoing.reshape(experts, capacity, width)
    arrived = lax.all_to_all(outgoing, ("sp", "tp"), split_axis=0, concat_axis=0, tiled=True)
    result = expert(arrived.reshape(-1, width), expert_gate, expert_up, expert_down)
    result = result.reshape(experts, capacity, width)
    returned = lax.all_to_all(result, ("sp", "tp"), split_axis=0, concat_axis=0, tiled=True)
    return collect(returned.reshape(-1, width), weights, resid)


def solution(mesh):
    in_specs = (
        P(("grp", "sp", "tp"), None),
        P(("grp", "sp"), "tp"),
        P(("grp", "sp"), "tp"),
        P(None, ("grp", "sp")),
        P(None, ("grp", "sp")),
        P(None, ("grp", "sp")),
        P(None, ("grp", "sp")),
        P("tp", ("grp", "sp")),
        P("tp", ("grp", "sp")),
        P("tp", None),
        P("tp", None),
        P(),
        P(("sp", "tp"), None, None),
        P(("sp", "tp"), None, None),
        P(("sp", "tp"), None, None),
        P(("grp", "sp", "tp"), None),
        P(("grp", "sp", "tp"), None),
    )
    out_specs = P(("grp", "sp", "tp"), None)

    return jax.shard_map(shards, mesh=mesh, in_specs=in_specs, out_specs=out_specs, check_vma=False)
```

```python
import math

import jax
import jax.numpy as jnp
from jax import lax
from jax.experimental import pallas as pl
from jax.experimental.pallas import tpu as pltpu
from jax.sharding import PartitionSpec as P


BF = jnp.bfloat16
F32 = jnp.float32
LOG2E = math.log2(math.e)
GATE_ROWS = 16
PIECES = 3
LOW = -1e30


def params(mib=16):
    return pltpu.CompilerParams(vmem_limit_bytes=mib << 20)


def packed(keys_values, gates, size_s, size_l, heads_s):
    at_l = size_s + GATE_ROWS
    at_v = at_l + size_l + GATE_ROWS

    def body(kv, gate, out):
        def pieces(left, size):
            left = left * -(size**0.5)
            rows = []
            for _ in range(PIECES):
                piece = left.astype(BF).astype(F32)
                rows.append(piece)
                left = left - piece
            used = PIECES * left.shape[0]
            rows.append(jnp.zeros((GATE_ROWS - used, left.shape[1]), F32))
            return jnp.concatenate(rows, axis=0).astype(BF)

        out[:size_s] = kv[:size_s]
        out[size_s:at_l] = pieces(gate[:heads_s], size_s)
        out[at_l : at_l + size_l] = kv[size_s : size_s + size_l]
        out[at_l + size_l : at_v] = pieces(gate[heads_s:], size_l)
        out[at_v:] = kv[size_s + size_l :]

    return pl.pallas_call(
        body,
        out_shape=jax.ShapeDtypeStruct((at_v + size_s + size_l, keys_values.shape[1]), BF),
        compiler_params=params(),
        name="packed",
    )(keys_values, gates)


def update(units, kind, keys, values, state, factor, keeps):
    rows = values.shape[1]
    tops = [state[g, h, rows : rows + 1] for _, g, h in units]

    def scores(i):
        queries, g, h = units[i]
        s = jnp.dot(keys[kind], queries[h], preferred_element_type=F32)
        return s if keeps is None else jnp.where(keeps[g], s, LOW)

    s = scores(0)
    for i, (_, g, h) in enumerate(units):
        following = scores(i + 1) if i + 1 < len(units) else None
        new = jnp.maximum(tops[i], jnp.max(s, axis=0, keepdims=True))
        p = jnp.exp2((s - new) * factor).astype(BF)
        alpha = jnp.exp2((tops[i] - new) * factor)
        mixed = jnp.dot(values[kind], p, preferred_element_type=F32)
        state[g, h, :rows] = state[g, h, :rows] * alpha + mixed
        state[g, h, rows:] = jnp.broadcast_to(new, (state.shape[2] - rows, new.shape[1]))
        s = following


def lay_out(blocks, keys, values, sizes):
    large = max(sizes)
    count = blocks[0].shape[1]
    at_k, at_v = 0, sum(sizes) + GATE_ROWS * len(sizes)
    for kind, size in enumerate(sizes):
        blank = jnp.zeros((large - size, count), BF)
        ones = jnp.ones((GATE_ROWS, count), BF)
        for i, block in enumerate(blocks):
            at = pl.ds(i * count, count)
            key, gates = block[at_k : at_k + size], block[at_k + size : at_k + size + GATE_ROWS]
            value = block[at_v : at_v + size]
            gap = [blank] if size < large else []
            keys[kind, at] = jnp.concatenate([key] + gap + [gates], axis=0).T
            values[kind, :, at] = jnp.concatenate([value] + gap + [ones], axis=0)
        at_k += size + GATE_ROWS
        at_v += size


def add_keys(groups, counts, sizes, keys, values, state, keeps=None, together=2):
    number = math.gcd(together, *counts)

    def some(i, carry):
        large = i * number >= counts[0]
        factor = jnp.where(large, LOG2E * sizes[1] ** -0.5, LOG2E * sizes[0] ** -0.5)
        units = [(queries, g, i * number + k) for k in range(number) for g, queries in enumerate(groups)]
        update(units, large.astype(jnp.int32), keys, values, state, factor, keeps)
        return carry

    lax.fori_loop(0, sum(counts) // number, some, 0)


def key_scratch(sizes, count):
    rows = max(sizes) + GATE_ROWS
    return [pltpu.VMEM((len(sizes), count, rows), BF), pltpu.VMEM((len(sizes), rows, count), BF)]


def first(info, own, peer, block, counts, sizes):
    tokens = own.shape[0]
    rows = max(sizes) + GATE_ROWS

    def body(info, own, peer, block, q_own, q_peer, state, keys, values):
        def spread(queries, out):
            at = h = 0
            for count, size in zip(counts, sizes):
                turned = queries[:, at : at + count * size].T
                row = lax.broadcasted_iota(jnp.int32, (GATE_ROWS, tokens), 0)
                for k in range(count):
                    chosen = (row % count == k) & (row < PIECES * count)
                    out[h, :size] = turned[k * size : (k + 1) * size]
                    if size < rows - GATE_ROWS:
                        out[h, size : rows - GATE_ROWS] = jnp.zeros((rows - GATE_ROWS - size, tokens), BF)
                    out[h, rows - GATE_ROWS :] = jnp.where(chosen, 1.0, 0.0).astype(BF)
                    h += 1
                at += count * size

        lay_out([block], keys, values, sizes)
        spread(own, q_own)
        spread(peer, q_peer)
        state[:, :, :rows] = jnp.zeros(state.shape[:2] + (rows, tokens), F32)
        state[:, :, rows:] = jnp.full(state.shape[:2] + (8, tokens), LOW, F32)
        shape = (block.shape[1], tokens)
        ahead = lax.broadcasted_iota(jnp.int32, shape, 1) - lax.broadcasted_iota(jnp.int32, shape, 0)
        keeps = [ahead >= 0, ahead >= jnp.where(info[0] == 1, -shape[0], shape[1])]
        add_keys([q_own, q_peer], counts, sizes, keys, values, state, keeps)

    vm = pl.BlockSpec(memory_space=pltpu.VMEM)
    heads = sum(counts)
    return pl.pallas_call(
        body,
        in_specs=[pl.BlockSpec(memory_space=pltpu.SMEM)] + [vm] * 3,
        out_specs=[vm] * 3,
        out_shape=[
            jax.ShapeDtypeStruct((heads, rows, tokens), BF),
            jax.ShapeDtypeStruct((heads, rows, tokens), BF),
            jax.ShapeDtypeStruct((2, heads, rows + 8, tokens), F32),
        ],
        scratch_shapes=key_scratch(sizes, block.shape[1]),
        compiler_params=params(),
        name="first",
    )(info, own, peer, block)


def advance(info, step, q_own, q_peer, blocks, state, counts, sizes):
    def body(flags, q_own, q_peer, *refs):
        arrived, state, keys, values = refs[: len(blocks)], refs[-3], refs[-2], refs[-1]

        @pl.when(flags[step] == 1)
        def _():
            lay_out(arrived, keys, values, sizes)
            add_keys([q_own, q_peer], counts, sizes, keys, values, state)

    vm = pl.BlockSpec(memory_space=pltpu.VMEM)
    return pl.pallas_call(
        body,
        in_specs=[pl.BlockSpec(memory_space=pltpu.SMEM)] + [vm] * (3 + len(blocks)),
        out_specs=vm,
        out_shape=jax.ShapeDtypeStruct(state.shape, state.dtype),
        input_output_aliases={3 + len(blocks): 0},
        scratch_shapes=key_scratch(sizes, sum(b.shape[1] for b in blocks)),
        compiler_params=params(),
    )(info, q_own, q_peer, *blocks, state)


def finish(state, got, project_s, project_l, counts, sizes):
    def body(state, got, project_s, project_l, out):
        rows = state.shape[2] - 8
        total, h = None, 0
        for count, size, project in zip(counts, sizes, (project_s, project_l)):
            factor = LOG2E * size**-0.5
            done = []
            for _ in range(count):
                a, b = state[0, h, rows : rows + 1], got[h, rows : rows + 1]
                top = jnp.maximum(a, b)
                wa, wb = jnp.exp2((a - top) * factor), jnp.exp2((b - top) * factor)
                norm = state[0, h, rows - 1 : rows] * wa + got[h, rows - 1 : rows] * wb
                done.append(((state[0, h, :size] * wa + got[h, :size] * wb) / norm).astype(BF))
                h += 1
            part = jnp.dot(jnp.concatenate(done, axis=0).T, project[...], preferred_element_type=F32)
            total = part if total is None else total + part
        out[...] = total.astype(BF)

    return pl.pallas_call(
        body,
        out_shape=jax.ShapeDtypeStruct((state.shape[3], project_s.shape[1]), BF),
        compiler_params=params(),
        name="finish",
    )(state, got, project_s, project_l)


def attend_and_project(qs, ql, key_small, key_large, value_small, value_large, gs, gl, ps, pb):
    devices = lax.axis_size("sp")
    chips = devices // 2
    place = lax.axis_index("sp").astype(jnp.int32)
    chip, core = place // 2, place % 2
    swap = [(i, i ^ 1) for i in range(devices)]
    ring = [(i, (i + 2 - 4 * (i % 2)) % devices) for i in range(devices)]
    steps = chips // 2
    k = jnp.arange(1, steps + 1, dtype=jnp.int32)
    usable = jnp.where(core == 0, chip >= k, chip + k >= chips).astype(jnp.int32)
    info = jnp.concatenate([(1 - core).reshape(1), usable])
    counts = (gs.shape[0], gl.shape[0])
    sizes = (key_small.shape[0], key_large.shape[0])

    kv = jnp.concatenate([key_small, key_large, value_small, value_large], axis=0)
    gates = jnp.concatenate([gs, gl], axis=0)
    block = packed(kv, gates, *sizes, counts[0])
    own = jnp.concatenate([qs, ql], axis=1)
    peer = lax.ppermute(own, "sp", swap)
    b = lax.ppermute(block, "sp", swap)
    a = block
    q_own, q_peer, state = first(info, own, peer, block, counts, sizes)
    for step in range(1, steps + 1):
        a = lax.ppermute(a, "sp", ring)
        blocks = [a]
        if step < steps or chips % 2:
            b = lax.ppermute(b, "sp", ring)
            blocks.append(b)
        state = advance(info, step, q_own, q_peer, blocks, state, counts, sizes)
    got = lax.ppermute(state[1], "sp", swap)
    return finish(state, got, ps, pb, counts, sizes)


def mix_body(parts, residual_in, gain, slots, resid_out, outgoing):
    projected = parts[0].astype(F32)
    for i in range(1, parts.shape[0]):
        projected = projected + parts[i].astype(F32)
    resid = residual_in[...].astype(F32) + projected
    resid_out[...] = resid
    scale = lax.rsqrt(jnp.mean(resid * resid, axis=1, keepdims=True) + 1e-06)
    normed = (resid * scale * gain[...].astype(F32)).astype(BF)
    outgoing[...] = jnp.dot(slots[...], normed, preferred_element_type=F32).astype(BF)


def mix(parts, residual_in, gain, slots):
    rows, width = residual_in.shape
    return pl.pallas_call(
        mix_body,
        out_shape=(
            jax.ShapeDtypeStruct((rows, width), F32),
            jax.ShapeDtypeStruct((slots.shape[0], width), BF),
        ),
        compiler_params=params(),
        name="mix",
    )(parts, residual_in, gain, slots)


def expert(rows, gate, up, down):
    count, width = rows.shape
    units = gate.shape[2]
    pieces = 4
    deep = width // pieces
    span = math.gcd(width, 512)

    def body(rows, gate, up, down, out, gate_v, up_v, down_v, g, u, hidden, sems):
        def inward(i):
            at = pl.ds(pl.multiple_of(i * deep, deep), deep)
            return (
                pltpu.make_async_copy(gate.at[0, at], gate_v.at[at], sems.at[2 * i]),
                pltpu.make_async_copy(up.at[0, at], up_v.at[at], sems.at[2 * i + 1]),
            )

        outward = pltpu.make_async_copy(down.at[0], down_v, sems.at[2 * pieces])
        for i in range(pieces):
            for copy in inward(i):
                copy.start()
        outward.start()
        g[...] = jnp.zeros_like(g)
        u[...] = jnp.zeros_like(u)

        def first_products(i, carry):
            at = pl.ds(pl.multiple_of(i * deep, deep), deep)
            for copy, weight, total in zip(inward(i), (gate_v, up_v), (g, u)):
                copy.wait()
                total[...] += jnp.dot(rows[:, at], weight[at], preferred_element_type=F32)
            return carry

        lax.fori_loop(0, pieces, first_products, 0)
        gated = g[...]
        hidden[...] = (gated / (1.0 + jnp.exp(-gated)) * u[...]).astype(BF)
        outward.wait()

        def last_product(i, carry):
            at = pl.ds(pl.multiple_of(i * span, span), span)
            out[:, at] = jnp.dot(hidden[...], down_v[:, at], preferred_element_type=F32).astype(BF)
            return carry

        lax.fori_loop(0, width // span, last_product, 0)

    vm = pl.BlockSpec(memory_space=pltpu.VMEM)
    return pl.pallas_call(
        body,
        in_specs=[vm] + [pl.BlockSpec(memory_space=pltpu.HBM)] * 3,
        out_specs=vm,
        out_shape=jax.ShapeDtypeStruct((count, width), BF),
        scratch_shapes=[
            pltpu.VMEM((width, units), BF),
            pltpu.VMEM((width, units), BF),
            pltpu.VMEM((units, width), BF),
            pltpu.VMEM((count, units), F32),
            pltpu.VMEM((count, units), F32),
            pltpu.VMEM((count, units), BF),
            pltpu.SemaphoreType.DMA((2 * pieces + 1,)),
        ],
        compiler_params=params(51),
        name="expert",
    )(rows, gate, up, down)


def collect_body(returned, weights, resid, out):
    total = resid[...]
    for i in range(weights.shape[0]):
        total = total + jnp.dot(weights[i], returned[...], preferred_element_type=F32)
    out[...] = total.astype(BF)


def collect(returned, weights, resid):
    return pl.pallas_call(
        collect_body,
        out_shape=jax.ShapeDtypeStruct(resid.shape, BF),
        compiler_params=params(),
        name="collect",
    )(returned, weights, resid)


def three_pieces(value):
    pieces = []
    for _ in range(PIECES):
        piece = lax.reduce_precision(value, 8, 7)
        pieces.append(piece.astype(BF))
        value = value - piece
    return jnp.stack(pieces)


def shards(
    residual_in,
    query_small,
    query_large,
    key_small,
    key_large,
    value_small,
    value_large,
    forget_small,
    forget_large,
    project_small,
    project_large,
    norm_gain,
    expert_gate,
    expert_up,
    expert_down,
    routing,
    route_weight,
):
    head_devices = lax.axis_size("tp")
    experts = lax.axis_size("sp") * head_devices
    own_rows, width = residual_in.shape
    top_count = routing.shape[1]

    partial = attend_and_project(
        query_small,
        query_large,
        key_small,
        key_large,
        value_small,
        value_large,
        forget_small,
        forget_large,
        project_small,
        project_large,
    )

    capacity = max(2, 2 * own_rows * top_count // experts)
    pairs = own_rows * top_count
    pair_expert = routing.reshape(-1)
    same = pair_expert[:, None] == pair_expert[None, :]
    before = jnp.arange(pairs)[:, None] > jnp.arange(pairs)[None, :]
    slot = jnp.sum((same & before).astype(jnp.int32), axis=1)
    target = (pair_expert * capacity + slot).reshape(own_rows, top_count)
    hit = target[:, :, None] == jnp.arange(experts * capacity)[None, None, :]
    slots = jnp.any(hit, axis=1).T.astype(BF)
    weights = three_pieces(jnp.sum(jnp.where(hit, route_weight[:, :, None], 0.0), axis=1))

    parts = partial.reshape(head_devices, own_rows, width)
    parts = lax.all_to_all(parts, "tp", split_axis=0, concat_axis=0, tiled=True)
    resid, outgoing = mix(parts, residual_in, norm_gain.reshape(1, width), slots)
    outgoing = outgoing.reshape(experts, capacity, width)
    arrived = lax.all_to_all(outgoing, ("sp", "tp"), split_axis=0, concat_axis=0, tiled=True)
    result = expert(arrived.reshape(-1, width), expert_gate, expert_up, expert_down)
    result = result.reshape(experts, capacity, width)
    returned = lax.all_to_all(result, ("sp", "tp"), split_axis=0, concat_axis=0, tiled=True)
    return collect(returned.reshape(-1, width), weights, resid)


def solution(mesh):
    in_specs = (
        P(("grp", "sp", "tp"), None),
        P(("grp", "sp"), "tp"),
        P(("grp", "sp"), "tp"),
        P(None, ("grp", "sp")),
        P(None, ("grp", "sp")),
        P(None, ("grp", "sp")),
        P(None, ("grp", "sp")),
        P("tp", ("grp", "sp")),
        P("tp", ("grp", "sp")),
        P("tp", None),
        P("tp", None),
        P(),
        P(("sp", "tp"), None, None),
        P(("sp", "tp"), None, None),
        P(("sp", "tp"), None, None),
        P(("grp", "sp", "tp"), None),
        P(("grp", "sp", "tp"), None),
    )
    out_specs = P(("grp", "sp", "tp"), None)

    return jax.shard_map(shards, mesh=mesh, in_specs=in_specs, out_specs=out_specs, check_vma=False)
```

```python
import math

import jax
import jax.numpy as jnp
from jax import lax
from jax.experimental import pallas as pl
from jax.experimental.pallas import tpu as pltpu
from jax.sharding import PartitionSpec as P


BF = jnp.bfloat16
F32 = jnp.float32
LOG2E = math.log2(math.e)
GATE_ROWS = 16
PIECES = 3
LOW = -1e30


def params(mib=16):
    return pltpu.CompilerParams(vmem_limit_bytes=mib << 20)


def packed(keys_values, gates, size_s, size_l, heads_s):
    at_l = size_s + GATE_ROWS
    at_v = at_l + size_l + GATE_ROWS

    def body(kv, gate, out):
        def pieces(left, size):
            left = left * -(size**0.5)
            rows = []
            for _ in range(PIECES):
                piece = left.astype(BF).astype(F32)
                rows.append(piece)
                left = left - piece
            used = PIECES * left.shape[0]
            rows.append(jnp.zeros((GATE_ROWS - used, left.shape[1]), F32))
            return jnp.concatenate(rows, axis=0).astype(BF)

        out[:size_s] = kv[:size_s]
        out[size_s:at_l] = pieces(gate[:heads_s], size_s)
        out[at_l : at_l + size_l] = kv[size_s : size_s + size_l]
        out[at_l + size_l : at_v] = pieces(gate[heads_s:], size_l)
        out[at_v:] = kv[size_s + size_l :]

    return pl.pallas_call(
        body,
        out_shape=jax.ShapeDtypeStruct((at_v + size_s + size_l, keys_values.shape[1]), BF),
        compiler_params=params(),
        name="packed",
    )(keys_values, gates)


def update(units, kind, keys, values, state, factor, keeps):
    rows = values.shape[1]
    tops = [state[g, h, rows : rows + 1] for _, g, h in units]

    def scores(i):
        queries, g, h = units[i]
        s = jnp.dot(keys[kind], queries[h], preferred_element_type=F32)
        return s if keeps is None else jnp.where(keeps[g], s, LOW)

    s = scores(0)
    for i, (_, g, h) in enumerate(units):
        following = scores(i + 1) if i + 1 < len(units) else None
        new = jnp.maximum(tops[i], jnp.max(s, axis=0, keepdims=True))
        p = jnp.exp2((s - new) * factor).astype(BF)
        alpha = jnp.exp2((tops[i] - new) * factor)
        mixed = jnp.dot(values[kind], p, preferred_element_type=F32)
        state[g, h, :rows] = state[g, h, :rows] * alpha + mixed
        state[g, h, rows:] = jnp.broadcast_to(new, (state.shape[2] - rows, new.shape[1]))
        s = following


def lay_out(blocks, keys, values, sizes):
    large = max(sizes)
    count = blocks[0].shape[1]
    at_k, at_v = 0, sum(sizes) + GATE_ROWS * len(sizes)
    for kind, size in enumerate(sizes):
        blank = jnp.zeros((large - size, count), BF)
        ones = jnp.ones((GATE_ROWS, count), BF)
        for i, block in enumerate(blocks):
            at = pl.ds(i * count, count)
            key, gates = block[at_k : at_k + size], block[at_k + size : at_k + size + GATE_ROWS]
            value = block[at_v : at_v + size]
            gap = [blank] if size < large else []
            keys[kind, at] = jnp.concatenate([key] + gap + [gates], axis=0).T
            values[kind, :, at] = jnp.concatenate([value] + gap + [ones], axis=0)
        at_k += size + GATE_ROWS
        at_v += size


def add_keys(groups, counts, sizes, keys, values, state, keeps=None, together=2):
    number = math.gcd(together, *counts)

    def some(i, carry):
        large = i * number >= counts[0]
        factor = jnp.where(large, LOG2E * sizes[1] ** -0.5, LOG2E * sizes[0] ** -0.5)
        units = [(queries, g, i * number + k) for k in range(number) for g, queries in enumerate(groups)]
        update(units, large.astype(jnp.int32), keys, values, state, factor, keeps)
        return carry

    lax.fori_loop(0, sum(counts) // number, some, 0)


def key_scratch(sizes, count):
    rows = max(sizes) + GATE_ROWS
    return [pltpu.VMEM((len(sizes), count, rows), BF), pltpu.VMEM((len(sizes), rows, count), BF)]


def first(info, own, peer, block, counts, sizes):
    tokens = own.shape[0]
    rows = max(sizes) + GATE_ROWS

    def body(info, own, peer, block, q_own, q_peer, state, keys, values):
        def spread(queries, out):
            at = h = 0
            for count, size in zip(counts, sizes):
                turned = queries[:, at : at + count * size].T
                row = lax.broadcasted_iota(jnp.int32, (GATE_ROWS, tokens), 0)
                for k in range(count):
                    chosen = (row % count == k) & (row < PIECES * count)
                    out[h, :size] = turned[k * size : (k + 1) * size]
                    if size < rows - GATE_ROWS:
                        out[h, size : rows - GATE_ROWS] = jnp.zeros((rows - GATE_ROWS - size, tokens), BF)
                    out[h, rows - GATE_ROWS :] = jnp.where(chosen, 1.0, 0.0).astype(BF)
                    h += 1
                at += count * size

        lay_out([block], keys, values, sizes)
        spread(own, q_own)
        spread(peer, q_peer)
        state[:, :, :rows] = jnp.zeros(state.shape[:2] + (rows, tokens), F32)
        state[:, :, rows:] = jnp.full(state.shape[:2] + (8, tokens), LOW, F32)
        shape = (block.shape[1], tokens)
        ahead = lax.broadcasted_iota(jnp.int32, shape, 1) - lax.broadcasted_iota(jnp.int32, shape, 0)
        keeps = [ahead >= 0, ahead >= jnp.where(info[0] == 1, -shape[0], shape[1])]
        add_keys([q_own, q_peer], counts, sizes, keys, values, state, keeps)

    vm = pl.BlockSpec(memory_space=pltpu.VMEM)
    heads = sum(counts)
    return pl.pallas_call(
        body,
        in_specs=[pl.BlockSpec(memory_space=pltpu.SMEM)] + [vm] * 3,
        out_specs=[vm] * 3,
        out_shape=[
            jax.ShapeDtypeStruct((heads, rows, tokens), BF),
            jax.ShapeDtypeStruct((heads, rows, tokens), BF),
            jax.ShapeDtypeStruct((2, heads, rows + 8, tokens), F32),
        ],
        scratch_shapes=key_scratch(sizes, block.shape[1]),
        compiler_params=params(),
        name="first",
    )(info, own, peer, block)


def advance(info, step, q_own, q_peer, blocks, state, counts, sizes):
    def body(flags, q_own, q_peer, *refs):
        arrived, state, keys, values = refs[: len(blocks)], refs[-3], refs[-2], refs[-1]

        @pl.when(flags[step] == 1)
        def _():
            lay_out(arrived, keys, values, sizes)
            add_keys([q_own, q_peer], counts, sizes, keys, values, state)

    vm = pl.BlockSpec(memory_space=pltpu.VMEM)
    return pl.pallas_call(
        body,
        in_specs=[pl.BlockSpec(memory_space=pltpu.SMEM)] + [vm] * (3 + len(blocks)),
        out_specs=vm,
        out_shape=jax.ShapeDtypeStruct(state.shape, state.dtype),
        input_output_aliases={3 + len(blocks): 0},
        scratch_shapes=key_scratch(sizes, sum(b.shape[1] for b in blocks)),
        compiler_params=params(),
    )(info, q_own, q_peer, *blocks, state)


def finish(state, got, project_s, project_l, counts, sizes):
    def body(state, got, project_s, project_l, out):
        rows = state.shape[2] - 8
        total, h = None, 0
        for count, size, project in zip(counts, sizes, (project_s, project_l)):
            factor = LOG2E * size**-0.5
            done = []
            for _ in range(count):
                a, b = state[0, h, rows : rows + 1], got[h, rows : rows + 1]
                top = jnp.maximum(a, b)
                wa, wb = jnp.exp2((a - top) * factor), jnp.exp2((b - top) * factor)
                norm = state[0, h, rows - 1 : rows] * wa + got[h, rows - 1 : rows] * wb
                done.append(((state[0, h, :size] * wa + got[h, :size] * wb) / norm).astype(BF))
                h += 1
            part = jnp.dot(jnp.concatenate(done, axis=0).T, project[...], preferred_element_type=F32)
            total = part if total is None else total + part
        out[...] = total.astype(BF)

    return pl.pallas_call(
        body,
        out_shape=jax.ShapeDtypeStruct((state.shape[3], project_s.shape[1]), BF),
        compiler_params=params(),
        name="finish",
    )(state, got, project_s, project_l)


def attend_and_project(qs, ql, key_small, key_large, value_small, value_large, gs, gl, ps, pb):
    devices = lax.axis_size("sp")
    chips = devices // 2
    place = lax.axis_index("sp").astype(jnp.int32)
    chip, core = place // 2, place % 2
    swap = [(i, i ^ 1) for i in range(devices)]
    ring = [(i, (i + 2 - 4 * (i % 2)) % devices) for i in range(devices)]
    steps = chips // 2
    k = jnp.arange(1, steps + 1, dtype=jnp.int32)
    usable = jnp.where(core == 0, chip >= k, chip + k >= chips).astype(jnp.int32)
    info = jnp.concatenate([(1 - core).reshape(1), usable])
    counts = (gs.shape[0], gl.shape[0])
    sizes = (key_small.shape[0], key_large.shape[0])

    kv = jnp.concatenate([key_small, key_large, value_small, value_large], axis=0)
    gates = jnp.concatenate([gs, gl], axis=0)
    block = packed(kv, gates, *sizes, counts[0])
    own = jnp.concatenate([qs, ql], axis=1)
    peer = lax.ppermute(own, "sp", swap)
    b = lax.ppermute(block, "sp", swap)
    a = block
    q_own, q_peer, state = first(info, own, peer, block, counts, sizes)
    for step in range(1, steps + 1):
        a = lax.ppermute(a, "sp", ring)
        blocks = [a]
        if step < steps or chips % 2:
            b = lax.ppermute(b, "sp", ring)
            blocks.append(b)
        state = advance(info, step, q_own, q_peer, blocks, state, counts, sizes)
    got = lax.ppermute(state[1], "sp", swap)
    return finish(state, got, ps, pb, counts, sizes)


def mix_body(parts, residual_in, gain, slots, resid_out, outgoing):
    projected = parts[0].astype(F32)
    for i in range(1, parts.shape[0]):
        projected = projected + parts[i].astype(F32)
    resid = residual_in[...].astype(F32) + projected
    resid_out[...] = resid
    scale = lax.rsqrt(jnp.mean(resid * resid, axis=1, keepdims=True) + 1e-06)
    normed = (resid * scale * gain[...].astype(F32)).astype(BF)
    outgoing[...] = jnp.dot(slots[...], normed, preferred_element_type=F32).astype(BF)


def mix(parts, residual_in, gain, slots):
    rows, width = residual_in.shape
    return pl.pallas_call(
        mix_body,
        out_shape=(
            jax.ShapeDtypeStruct((rows, width), F32),
            jax.ShapeDtypeStruct((slots.shape[0], width), BF),
        ),
        compiler_params=params(),
        name="mix",
    )(parts, residual_in, gain, slots)


def expert(rows, gate, up, down):
    count, width = rows.shape
    units = gate.shape[2]
    pieces = 4
    deep = width // pieces
    span = math.gcd(width, 512)

    def body(rows, gate, up, down, out, gate_v, up_v, down_v, g, u, hidden, sems):
        def inward(i):
            at = pl.ds(pl.multiple_of(i * deep, deep), deep)
            return (
                pltpu.make_async_copy(gate.at[0, at], gate_v.at[at], sems.at[2 * i]),
                pltpu.make_async_copy(up.at[0, at], up_v.at[at], sems.at[2 * i + 1]),
            )

        outward = pltpu.make_async_copy(down.at[0], down_v, sems.at[2 * pieces])
        for i in range(pieces):
            for copy in inward(i):
                copy.start()
        outward.start()
        g[...] = jnp.zeros_like(g)
        u[...] = jnp.zeros_like(u)

        def first_products(i, carry):
            at = pl.ds(pl.multiple_of(i * deep, deep), deep)
            for copy, weight, total in zip(inward(i), (gate_v, up_v), (g, u)):
                copy.wait()
                total[...] += jnp.dot(rows[:, at], weight[at], preferred_element_type=F32)
            return carry

        lax.fori_loop(0, pieces, first_products, 0)
        gated = g[...]
        hidden[...] = (gated / (1.0 + jnp.exp(-gated)) * u[...]).astype(BF)
        outward.wait()

        def last_product(i, carry):
            at = pl.ds(pl.multiple_of(i * span, span), span)
            out[:, at] = jnp.dot(hidden[...], down_v[:, at], preferred_element_type=F32).astype(BF)
            return carry

        lax.fori_loop(0, width // span, last_product, 0)

    vm = pl.BlockSpec(memory_space=pltpu.VMEM)
    return pl.pallas_call(
        body,
        in_specs=[vm] + [pl.BlockSpec(memory_space=pltpu.HBM)] * 3,
        out_specs=vm,
        out_shape=jax.ShapeDtypeStruct((count, width), BF),
        scratch_shapes=[
            pltpu.VMEM((width, units), BF),
            pltpu.VMEM((width, units), BF),
            pltpu.VMEM((units, width), BF),
            pltpu.VMEM((count, units), F32),
            pltpu.VMEM((count, units), F32),
            pltpu.VMEM((count, units), BF),
            pltpu.SemaphoreType.DMA((2 * pieces + 1,)),
        ],
        compiler_params=params(51),
        name="expert",
    )(rows, gate, up, down)


def collect_body(returned, weights, resid, out):
    total = resid[...]
    for i in range(weights.shape[0]):
        total = total + jnp.dot(weights[i], returned[...], preferred_element_type=F32)
    out[...] = total.astype(BF)


def collect(returned, weights, resid):
    return pl.pallas_call(
        collect_body,
        out_shape=jax.ShapeDtypeStruct(resid.shape, BF),
        compiler_params=params(),
        name="collect",
    )(returned, weights, resid)


def three_pieces(value):
    pieces = []
    for _ in range(PIECES):
        piece = lax.reduce_precision(value, 8, 7)
        pieces.append(piece.astype(BF))
        value = value - piece
    return jnp.stack(pieces)


def shards(
    residual_in,
    query_small,
    query_large,
    key_small,
    key_large,
    value_small,
    value_large,
    forget_small,
    forget_large,
    project_small,
    project_large,
    norm_gain,
    expert_gate,
    expert_up,
    expert_down,
    routing,
    route_weight,
):
    head_devices = lax.axis_size("tp")
    experts = lax.axis_size("sp") * head_devices
    own_rows, width = residual_in.shape
    top_count = routing.shape[1]

    partial = attend_and_project(
        query_small,
        query_large,
        key_small,
        key_large,
        value_small,
        value_large,
        forget_small,
        forget_large,
        project_small,
        project_large,
    )

    capacity = max(2, 2 * own_rows * top_count // experts)
    pairs = own_rows * top_count
    gain = norm_gain.reshape(1, width)
    pair_expert = (routing * capacity).reshape(-1)
    same = pair_expert[:, None] == pair_expert[None, :]
    before = jnp.arange(pairs)[:, None] > jnp.arange(pairs)[None, :]
    slot = jnp.sum((same & before).astype(jnp.int32), axis=1)
    target = (pair_expert + slot).reshape(own_rows, top_count)
    hit = target[:, :, None] == jnp.arange(experts * capacity)[None, None, :]
    slots = jnp.any(hit, axis=1).T.astype(BF)
    weights = three_pieces(jnp.sum(jnp.where(hit, route_weight[:, :, None], 0.0), axis=1))
    slots, weights = lax.optimization_barrier((slots, weights))

    parts = partial.reshape(head_devices, own_rows, width)
    parts = lax.all_to_all(parts, "tp", split_axis=0, concat_axis=0, tiled=True)
    resid, outgoing = mix(parts, residual_in, gain, slots)
    outgoing = outgoing.reshape(experts, capacity, width)
    arrived = lax.all_to_all(outgoing, ("sp", "tp"), split_axis=0, concat_axis=0, tiled=True)
    result = expert(arrived.reshape(-1, width), expert_gate, expert_up, expert_down)
    result = result.reshape(experts, capacity, width)
    returned = lax.all_to_all(result, ("sp", "tp"), split_axis=0, concat_axis=0, tiled=True)
    return collect(returned.reshape(-1, width), weights, resid)


def solution(mesh):
    in_specs = (
        P(("grp", "sp", "tp"), None),
        P(("grp", "sp"), "tp"),
        P(("grp", "sp"), "tp"),
        P(None, ("grp", "sp")),
        P(None, ("grp", "sp")),
        P(None, ("grp", "sp")),
        P(None, ("grp", "sp")),
        P("tp", ("grp", "sp")),
        P("tp", ("grp", "sp")),
        P("tp", None),
        P("tp", None),
        P(),
        P(("sp", "tp"), None, None),
        P(("sp", "tp"), None, None),
        P(("sp", "tp"), None, None),
        P(("grp", "sp", "tp"), None),
        P(("grp", "sp", "tp"), None),
    )
    out_specs = P(("grp", "sp", "tp"), None)

    return jax.shard_map(shards, mesh=mesh, in_specs=in_specs, out_specs=out_specs, check_vma=False)
```
